32 devices in a mesh: ep: 8 (over z, y), tp: 4 (over x, core).
Axes of the slice: x: 2, y: 2, z: 4, core: 2. Of those that a mesh axis runs over, the one named last changes fastest.
Arguments:
- tokens: bfloat16 [192, 1024], P('ep'), may hold values from -3 to 3
- attn_gain: float32 [1024], replicated, may hold values from 0.1 to 1.9
- w_query: bfloat16 [1024, 1024], P(None, 'tp'), may hold values from -0.1875 to 0.1875
- w_key: bfloat16 [1024, 256], P(None, 'tp'), may hold values from -0.1875 to 0.1875
- w_value: bfloat16 [1024, 256], P(None, 'tp'), may hold values from -0.1875 to 0.1875
- attn_bias: float32 [16], P('tp'), may hold values from -7.5 to -3
- key_cache: bfloat16 [192, 256, 1024], P('ep', 'tp'), may hold values from -6 to 6
- value_cache: bfloat16 [192, 256, 1024], P('ep', 'tp'), may hold values from -6 to 6
- lengths: int32 [192], P('ep'), may hold values from 128 to 1024
- w_out: bfloat16 [1024, 1024], P('tp'), may hold values from -0.75 to 0.75
- ffn_gain: float32 [1024], replicated, may hold values from 0.1 to 1.9
- routes: int32 [192, 2], P('ep'), may hold values from 0 to 7, all different within a row; in each aligned block of 24 rows (0 to 23, 24 to 47, ...) at most 12 rows name the same one
- route_weight: float32 [192, 2], P('ep'), may hold values from 0.2 to 1
- expert_gate: bfloat16 [8, 1024, 3584], P('ep', None, 'tp'), may hold values from -0.1875 to 0.1875
- expert_up: bfloat16 [8, 1024, 3584], P('ep', None, 'tp'), may hold values from -0.1875 to 0.1875
- expert_down: bfloat16 [8, 3584, 1024], P('ep', 'tp'), may hold values from -0.09375 to 0.09375
Outputs:
- mixed: bfloat16 [192, 1024], P('ep')
- new_keys: bfloat16 [192, 256], P('ep', 'tp')
- new_values: bfloat16 [192, 256], P('ep', 'tp')
The draws below stay inside these ranges and needn't reach their ends.
Inputs may be any that keep to these rules, and one draw needn't show every extreme that they name: `routes`: each row names 2 different experts. Among the rows of one device no expert is named by more than 12 of them, and on some device some expert is named by exactly 12.
All inputs are finite; a program needn't handle non-finite values.
Results may differ from the reference program's by a relative error of at most 0.02.
Values may be sent and summed in bfloat16 or wider, within the bound.
No kernel may reach another device: no remote copies, remote signals or barrier semaphores. Data moves between devices by JAX's collectives and lax.ppermute only.
A program may use at most 64 MiB of HBM per device.

```python
import math
import jax
import jax.numpy as jnp
import numpy as np
from jax import lax

D = 1024
HEADS = 16
KV_HEADS = 4
HEAD = 64
FF = 3584
TOP = 2
SEQS = 24
LEN = 1024
EXPERTS = 8
CAP = 12
BATCH = 192
N_EP = 8
N_TP = 4


def set_ends(drawn, stream_key, least, top_value):
    dims = drawn.shape
    index_at = [jax.random.randint(jax.random.fold_in(stream_key, axis), (), 0, dims[axis]) for axis in range(len(dims))]
    drawn = drawn.at[tuple(index_at)].set(least)
    longest = dims.index(max(dims))
    index_at[longest] = (index_at[longest] + 1) % dims[longest]
    return drawn.at[tuple(index_at)].set(top_value)


def level_of(stream_key, dims, cuts, low, high):
    def one(dim, shards_of):
        steps = jax.random.uniform(jax.random.fold_in(jax.random.fold_in(stream_key, 6), dim), (shards_of,), jnp.float32, low / len(cuts), high / len(cuts))
        return jnp.repeat(jnp.exp(steps), dims[dim] // shards_of).reshape((-1,) + (1,) * (len(dims) - dim - 1))

    factor_of = one(*cuts[0])
    for cut in cuts[1:]:
        factor_of = factor_of * one(*cut)
    return factor_of


def routed_block(rng, own, number, rows, number_of, top, limit, lean):
    order = jax.random.permutation(rng, number_of)
    heavy_load, usual = shares(number_of, rows * top, limit, lean, True), shares(number_of, rows * top, limit, lean, False)
    places = jnp.arange(number_of)

    def named(sizes, offset_by):
        used = int((sizes > 0).sum())
        fixed = max(1, used // 4)
        passed = fixed + (places - fixed + offset_by * (used - fixed)) % max(1, number_of - fixed)
        return jnp.zeros((number_of,), jnp.int32).at[order[jnp.where(places < fixed, places, passed)]].set(jnp.asarray(sizes, jnp.int32))

    sizes = jnp.where(number % 4 == 0, named(heavy_load, number // 4), named(usual, number - number // 4 - 1))
    mixed = jax.random.permutation(jax.random.fold_in(own, 3), number_of)
    donor, sink = mixed[0:number_of // 2 * 2:2], mixed[1:number_of // 2 * 2:2]
    margin = jnp.minimum(sizes[donor] - 1, limit - sizes[sink]) // 2
    margin = jnp.where((donor == order[0]) | (sink == order[0]) | (sizes[sink] == 0), 0, jnp.maximum(margin, 0))
    passed = jax.random.randint(jax.random.fold_in(own, 4), (number_of // 2,), 0, 1 << 20) % (margin + 1)
    sizes = sizes.at[donor].add(-passed).at[sink].add(passed)
    labels = jnp.searchsorted(jnp.cumsum(sizes), jnp.arange(rows * top), side="right").astype(jnp.int32)
    grid = labels.reshape(top, rows).T
    grid = grid[jax.random.permutation(jax.random.fold_in(own, 1), rows)]
    offset_by = jax.random.randint(jax.random.fold_in(own, 2), (rows, 1), 0, top)
    return jnp.take_along_axis(grid, (jnp.arange(top)[None, :] + offset_by) % top, axis=1)


def shares(amount, total, bound, skew, full):
    portions = [(1 << 20) // math.isqrt(rank ** skew) + 1 for rank in range(1, amount + 1)]
    largest = bound if full else min(bound, max(-(-total // amount), total * portions[0] // sum(portions)))
    least = 1 if total - largest >= amount - 1 else 0
    given, surplus = [largest] + [least] * (amount - 1), total - largest - least * (amount - 1)
    while surplus > 0:
        movable = [i for i in range(1, amount) if given[i] < largest] or [i for i in range(1, amount) if given[i] < bound]
        whole, remaining = sum([portions[i] for i in movable]), surplus
        for i in movable:
            extra = min(bound - given[i], max(1, remaining * portions[i] // whole), surplus)
            given[i] = given[i] + extra
            surplus = surplus - extra
    return np.array(given)


def normal_values(key, shape, scale, most, shards=(), kind=jnp.bfloat16):
    array = scale * jax.random.normal(key, shape, jnp.float32)
    if shards:
        array = array * level_of(key, shape, shards, -0.22, 0.18)
    return jnp.clip(array, -most, most).astype(kind)


def setup_inputs(seed: int = 0) -> dict:
    keys = jax.random.split(jax.random.key(seed), 17)
    tokens = normal_values(keys[0], (BATCH, D), 0.5, 3.0, ((0, 8),))
    attn_gain = jnp.clip(1.0 + 0.18 * jax.random.normal(keys[1], (D,), jnp.float32), 0.1, 1.9)
    w_query = normal_values(keys[2], (D, HEADS * HEAD), D ** -0.5, 0.1875, ((1, 4),))
    w_key = normal_values(keys[3], (D, KV_HEADS * HEAD), D ** -0.5, 0.1875, ((1, 4),))
    w_value = normal_values(keys[4], (D, KV_HEADS * HEAD), D ** -0.5, 0.1875, ((1, 4),))
    attn_bias = jnp.clip(-7.5 + 4.5 * jax.random.uniform(keys[5], (HEADS,), jnp.float32) ** level_of(keys[5], (HEADS,), ((0, 4),), -0.2, 0.2), -7.5, -3.0)
    key_cache = normal_values(keys[6], (BATCH, KV_HEADS * HEAD, LEN), 1.0, 6.0, ((0, 8), (1, 4)))
    value_cache = normal_values(keys[7], (BATCH, KV_HEADS * HEAD, LEN), 1.0, 6.0, ((0, 8), (1, 4)))
    lengths = set_ends(jax.random.randint(keys[8], (BATCH,), LEN // 8, LEN + 1), jax.random.fold_in(keys[8], 1), LEN // 8, LEN).astype(jnp.int32)
    w_out = normal_values(keys[9], (HEADS * HEAD, D), (HEADS * HEAD // 16) ** -0.5, 0.75, ((0, 4),))
    ffn_gain = jnp.clip(1.0 + 0.18 * jax.random.normal(keys[10], (D,), jnp.float32), 0.1, 1.9)
    routes_keys = jax.random.split(jax.random.fold_in(keys[11], 1), BATCH // SEQS)
    routes_turns = jax.random.permutation(jax.random.fold_in(keys[11], 3), BATCH // SEQS)
    routes = jax.vmap(lambda own, number: routed_block(jax.random.fold_in(keys[11], 2), own, number, SEQS, EXPERTS, TOP, CAP, 1))(routes_keys, routes_turns).reshape((BATCH, TOP))
    route_weight = jnp.clip(0.2 + 0.8 * jax.random.uniform(keys[12], (BATCH, TOP), jnp.float32) ** level_of(keys[12], (BATCH, TOP), ((0, 8),), -0.2, 0.2), 0.2, 1.0)
    expert_gate = normal_values(keys[13], (EXPERTS, D, FF), D ** -0.5, 0.1875, ((0, 8), (2, 4)))
    expert_up = normal_values(keys[14], (EXPERTS, D, FF), D ** -0.5, 0.1875, ((0, 8), (2, 4)))
    expert_down = normal_values(keys[15], (EXPERTS, FF, D), FF ** -0.5, 0.09375, ((0, 8), (1, 4)))
    return {"tokens": tokens, "attn_gain": attn_gain, "w_query": w_query, "w_key": w_key, "w_value": w_value, "attn_bias": attn_bias, "key_cache": key_cache, "value_cache": value_cache, "lengths": lengths, "w_out": w_out, "ffn_gain": ffn_gain, "routes": routes, "route_weight": route_weight, "expert_gate": expert_gate, "expert_up": expert_up, "expert_down": expert_down}


norm_epsilon = 1e-06

def rms_scale(inputs, gains):
    widened = inputs.astype(jnp.float32)
    factor = lax.rsqrt(lax.optimization_barrier(jnp.mean(widened * widened, axis=-1, keepdims=True)) + norm_epsilon)
    return (widened * factor * gains).astype(jnp.bfloat16)

def dispatch_matrix(block_routes, experts, capacity):
    flat_routes = block_routes.reshape(-1).astype(jnp.int32)
    onehot = (flat_routes[:, None] == jnp.arange(experts, dtype=jnp.int32)[None, :]).astype(jnp.int32)
    before = (jnp.cumsum(onehot, axis=0) - onehot).astype(jnp.int32)
    slot_index = lax.optimization_barrier(jnp.sum(before * onehot, axis=1)).astype(jnp.int32)
    target = flat_routes * capacity + slot_index
    return jnp.arange(experts * capacity, dtype=jnp.int32)[:, None] == target[None, :]

def stick_read(queries, key_block, value_block, bias_grid, lengths):
    row_count, kv_count, group_size, head_size = queries.shape
    key_span = key_block.shape[2]
    key_heads = key_block.reshape(row_count, kv_count, head_size, key_span).astype(jnp.float32)
    value_heads = value_block.reshape(row_count, kv_count, head_size, key_span).astype(jnp.float32)
    scores = jnp.einsum('skgd,skdl->skgl', queries.astype(jnp.float32), key_heads) * head_size ** (-0.5)
    scores = scores + bias_grid[None, :, :, None]
    inside = (jnp.arange(key_span, dtype=jnp.int32)[None, :] < lengths[:, None])[:, None, None, :]
    log_fall = jnp.where(inside, jax.nn.log_sigmoid(-scores), 0.0)
    log_after = lax.cumsum(log_fall, axis=3, reverse=True) - log_fall
    weights = jnp.where(inside, jnp.exp(jax.nn.log_sigmoid(scores) + log_after), 0.0).astype(jnp.bfloat16)
    mixed_out = jnp.einsum('skgl,skdl->skgd', weights.astype(jnp.float32), value_heads)
    return mixed_out.astype(jnp.bfloat16).reshape(row_count, -1)

def expert_rows(operands):
    row_block, gate_matrix, up_matrix, down_matrix = operands
    gate_act = jnp.dot(row_block, gate_matrix, preferred_element_type=jnp.float32)
    lifted = jnp.dot(row_block, up_matrix, preferred_element_type=jnp.float32)
    hidden = (jax.nn.silu(gate_act) * lifted).astype(jnp.bfloat16)
    pieces = jnp.einsum('rtf,tfd->rtd', hidden.reshape(hidden.shape[0], N_TP, -1).astype(jnp.float32), down_matrix.reshape(N_TP, -1, down_matrix.shape[1]).astype(jnp.float32))
    rounded = lax.optimization_barrier(pieces.astype(jnp.bfloat16))
    return lax.optimization_barrier(jnp.sum(rounded.astype(jnp.float32), axis=1)).astype(jnp.bfloat16)

def block_plan(block_routes):
    return dispatch_matrix(block_routes, EXPERTS, CAP)

def reference(tokens, attn_gain, w_query, w_key, w_value, attn_bias, key_cache, value_cache, lengths, w_out, ffn_gain, routes, route_weight, expert_gate, expert_up, expert_down):
    normed = rms_scale(tokens, attn_gain)
    queries = jnp.dot(normed, w_query, preferred_element_type=jnp.float32).astype(jnp.bfloat16)
    new_keys = jnp.dot(normed, w_key, preferred_element_type=jnp.float32).astype(jnp.bfloat16)
    new_values = jnp.dot(normed, w_value, preferred_element_type=jnp.float32).astype(jnp.bfloat16)
    group_size = HEADS // KV_HEADS
    grouped = queries.reshape(N_EP, SEQS, KV_HEADS, group_size, HEAD)
    bias_grid = attn_bias.reshape(KV_HEADS, group_size)

    def per_block(block_args):
        return stick_read(block_args[0], block_args[1], block_args[2], bias_grid, block_args[3])
    attended = lax.map(per_block, (grouped, key_cache.reshape(N_EP, SEQS, KV_HEADS * HEAD, LEN), value_cache.reshape(N_EP, SEQS, KV_HEADS * HEAD, LEN), lengths.reshape(N_EP, SEQS)))
    attended = attended.reshape(BATCH, HEADS * HEAD)
    parts = jnp.einsum('btf,tfd->btd', attended.reshape(BATCH, N_TP, -1).astype(jnp.float32), w_out.reshape(N_TP, -1, D).astype(jnp.float32))
    rounded = lax.optimization_barrier(parts.astype(jnp.bfloat16))
    attn_total = lax.optimization_barrier(jnp.sum(rounded.astype(jnp.float32), axis=1))
    residual = (tokens.astype(jnp.float32) + attn_total).astype(jnp.bfloat16)
    normed_two = rms_scale(residual, ffn_gain)
    plans = jax.vmap(block_plan)(routes.reshape(N_EP, SEQS, TOP)).astype(jnp.float32)
    repeated = jnp.repeat(normed_two.reshape(N_EP, SEQS, 1, D), TOP, axis=2).reshape(N_EP, SEQS * TOP, D)
    sent = jnp.einsum('per,prd->ped', plans, repeated.astype(jnp.float32)).astype(jnp.bfloat16)
    received = sent.reshape(N_EP, EXPERTS, CAP, D).transpose(1, 0, 2, 3).reshape(EXPERTS, N_EP * CAP, D)
    outputs = lax.map(expert_rows, (received, expert_gate, expert_up, expert_down))
    back = outputs.reshape(EXPERTS, N_EP, CAP, D).transpose(1, 0, 2, 3).reshape(N_EP, EXPERTS * CAP, D)
    picked = jnp.einsum('per,ped->prd', plans, back.astype(jnp.float32)).reshape(BATCH, TOP, D)
    moe_sum = lax.optimization_barrier(jnp.sum(picked * route_weight[:, :, None], axis=1))
    mixed = (residual.astype(jnp.float32) + moe_sum).astype(jnp.bfloat16)
    return (mixed, new_keys, new_values)
```

```python
import math

import jax
import jax.numpy as jnp
from jax import lax
from jax.sharding import PartitionSpec as P

HEADS = 16
KV_HEADS = 4
HEAD = 64


norm_epsilon = 1e-06


def rms_scale(inputs, gains):
    widened = inputs.astype(jnp.float32)
    factor = lax.rsqrt(jnp.mean(widened * widened, axis=-1, keepdims=True) + norm_epsilon)
    return (widened * factor * gains).astype(jnp.bfloat16)


def dispatch_matrix(block_routes, experts, capacity):
    flat_routes = block_routes.reshape(-1)
    onehot = (flat_routes[:, None] == jnp.arange(experts, dtype=jnp.int32)[None, :]).astype(
        jnp.float32
    )
    row_total = flat_routes.shape[0]
    row_ids = jnp.arange(row_total, dtype=jnp.int32)
    earlier = (row_ids[None, :] < row_ids[:, None]).astype(jnp.float32)
    before = jnp.dot(earlier, onehot, precision=lax.Precision.HIGHEST)
    slot_index = jnp.sum(before * onehot, axis=1).astype(jnp.int32)
    target = flat_routes * capacity + slot_index
    return jnp.arange(experts * capacity, dtype=jnp.int32)[:, None] == target[None, :]


def suffix_totals(log_fall):
    lead_shape = log_fall.shape[:-1]
    key_span = log_fall.shape[-1]
    block_len = math.gcd(key_span, 128)
    block_count = key_span // block_len
    blocked = log_fall.reshape(lead_shape + (block_count, block_len))
    inner_ids = jnp.arange(block_len, dtype=jnp.int32)
    upper_mask = (inner_ids[:, None] >= inner_ids[None, :]).astype(jnp.float32)
    within = jnp.einsum("...bj,ji->...bi", blocked, upper_mask, precision=lax.Precision.HIGHEST)
    block_sums = jnp.sum(blocked, axis=-1)
    block_ids = jnp.arange(block_count, dtype=jnp.int32)
    later_mask = (block_ids[:, None] > block_ids[None, :]).astype(jnp.float32)
    later = jnp.einsum("...c,cb->...b", block_sums, later_mask, precision=lax.Precision.HIGHEST)
    return (within + later[..., None]).reshape(lead_shape + (key_span,))


def stick_read(queries, key_block, value_block, bias_grid, lengths):
    row_count, kv_count, group_size, head_size = queries.shape
    key_span = key_block.shape[2]
    key_heads = key_block.reshape(row_count, kv_count, head_size, key_span)
    value_heads = value_block.reshape(row_count, kv_count, head_size, key_span)
    scores = jnp.einsum("skgd,skdl->skgl", queries, key_heads, preferred_element_type=jnp.float32)
    scores = scores * head_size ** (-0.5) + bias_grid[None, :, :, None]
    inside = (jnp.arange(key_span, dtype=jnp.int32)[None, :] < lengths[:, None])[:, None, None, :]
    log_fall = jnp.where(inside, jax.nn.log_sigmoid(-scores), 0.0)
    log_after = suffix_totals(log_fall) - log_fall
    weights = jnp.where(inside, jnp.exp(jax.nn.log_sigmoid(scores) + log_after), 0.0).astype(
        jnp.bfloat16
    )
    mixed_out = jnp.einsum(
        "skgl,skdl->skgd", weights, value_heads, preferred_element_type=jnp.float32
    )
    return mixed_out.astype(jnp.bfloat16).reshape(row_count, -1)


def tp_total(part):
    size = lax.axis_size("tp")
    step = 1
    while step < size:
        swap = [(i, i ^ step) for i in range(size)]
        other = lax.ppermute(part, "tp", swap)
        part = part.astype(jnp.float32) + other.astype(jnp.float32)
        step *= 2
        if step < size:
            part = part.astype(jnp.bfloat16)
    return part


def body(
    tokens,
    attn_gain,
    w_query,
    w_key,
    w_value,
    attn_bias,
    key_cache,
    value_cache,
    lengths,
    w_out,
    ffn_gain,
    routes,
    route_weight,
    expert_gate,
    expert_up,
    expert_down,
):
    seq_count, model_width = tokens.shape
    normed = rms_scale(tokens, attn_gain)
    queries = jnp.dot(normed, w_query, preferred_element_type=jnp.float32).astype(jnp.bfloat16)
    new_keys = jnp.dot(normed, w_key, preferred_element_type=jnp.float32).astype(jnp.bfloat16)
    new_values = jnp.dot(normed, w_value, preferred_element_type=jnp.float32).astype(jnp.bfloat16)
    kv_local = w_key.shape[1] // HEAD
    group_size = HEADS // KV_HEADS
    grouped = queries.reshape(seq_count, kv_local, group_size, HEAD)
    bias_grid = attn_bias.reshape(kv_local, group_size)
    attended = stick_read(grouped, key_cache, value_cache, bias_grid, lengths)
    partial_out = jnp.dot(attended, w_out, preferred_element_type=jnp.float32)
    attn_total = tp_total(partial_out.astype(jnp.bfloat16))
    residual = (tokens.astype(jnp.float32) + attn_total).astype(jnp.bfloat16)
    normed_two = rms_scale(residual, ffn_gain)
    expert_count = lax.axis_size("ep")
    top_count = routes.shape[1]
    capacity = max(2, 2 * seq_count * top_count // expert_count)
    route_plan = dispatch_matrix(routes, expert_count, capacity).astype(jnp.bfloat16)
    repeated = jnp.repeat(normed_two, top_count, axis=0)
    outgoing = jnp.dot(route_plan, repeated, preferred_element_type=jnp.float32).astype(
        jnp.bfloat16
    )
    outgoing = outgoing.reshape(expert_count, capacity, model_width)
    gate_local = expert_gate[0]
    up_local = expert_up[0]
    down_local = expert_down[0]
    arrived = lax.all_to_all(outgoing, "ep", split_axis=0, concat_axis=0, tiled=True)
    sources, slot_count, row_width = arrived.shape
    row_block = arrived.reshape(sources * slot_count, row_width)
    gate_act = jnp.dot(row_block, gate_local, preferred_element_type=jnp.float32)
    lifted = jnp.dot(row_block, up_local, preferred_element_type=jnp.float32)
    hidden = (jax.nn.silu(gate_act) * lifted).astype(jnp.bfloat16)
    partial_value = jnp.dot(hidden, down_local, preferred_element_type=jnp.float32)
    returned = lax.all_to_all(
        partial_value.astype(jnp.bfloat16).reshape(sources, slot_count, row_width),
        "ep",
        split_axis=0,
        concat_axis=0,
        tiled=True,
    )
    flat_back = returned.reshape(expert_count * capacity, row_width)
    picked = jnp.dot(route_plan.T, flat_back, preferred_element_type=jnp.float32)
    picked = picked.reshape(seq_count, top_count, row_width)
    moe_part = jnp.sum(picked * route_weight[:, :, None], axis=1).astype(jnp.bfloat16)
    mixed_rows = (residual.astype(jnp.float32) + tp_total(moe_part)).astype(jnp.bfloat16)
    return (mixed_rows, new_keys, new_values)


def solution(mesh):
    return jax.shard_map(
        body,
        mesh=mesh,
        in_specs=(
            P("ep", None),
            P(),
            P(None, "tp"),
            P(None, "tp"),
            P(None, "tp"),
            P("tp"),
            P("ep", "tp", None),
            P("ep", "tp", None),
            P("ep"),
            P("tp", None),
            P(),
            P("ep", None),
            P("ep", None),
            P("ep", None, "tp"),
            P("ep", None, "tp"),
            P("ep", "tp", None),
        ),
        out_specs=(P("ep", None), P("ep", "tp"), P("ep", "tp")),
        check_vma=False,
    )
```

```python
import functools

import jax
import jax.numpy as jnp
from jax import lax
from jax.experimental import pallas as pl
from jax.experimental.pallas import tpu as pltpu
from jax.sharding import PartitionSpec as P

HEAD = 64
norm_epsilon = 1e-06

LAST = (((1,), (1,)), ((), ()))


def iota(shape, axis):
    return lax.broadcasted_iota(jnp.int32, shape, axis)


def dot(a, b):
    return jnp.dot(a, b, preferred_element_type=jnp.float32)


def dot_last(a, b):
    return lax.dot_general(a, b, LAST, preferred_element_type=jnp.float32)


def attend_kernel(
    group,
    lengths,
    bias,
    tokens_hbm,
    gain_hbm,
    wq_hbm,
    wk_hbm,
    wv_hbm,
    wo_hbm,
    key_hbm,
    value_hbm,
    part_ref,
    new_key_ref,
    new_value_ref,
    tokens_ref,
    gain_ref,
    wq_ref,
    wk_ref,
    wv_ref,
    wo_ref,
    key_ref,
    value_ref,
    small_sem,
    key_sem,
    value_sem,
):
    seqs = tokens_ref.shape[0]
    span = key_ref.shape[1]
    heads = wq_ref.shape[1] // HEAD
    depth = group * HEAD
    rows = group * heads
    count = seqs // group
    fetched = [
        pltpu.make_async_copy(src, dst, small_sem.at[i])
        for i, (src, dst) in enumerate(
            (
                (tokens_hbm, tokens_ref),
                (gain_hbm, gain_ref),
                (wq_hbm, wq_ref),
                (wk_hbm, wk_ref),
                (wv_hbm, wv_ref),
                (wo_hbm, wo_ref),
            )
        )
    ]
    key_copies, value_copies = [], []
    for g in range(count):
        part = pl.ds(g * depth, depth)
        key_copies.append(
            pltpu.make_async_copy(key_hbm.at[part], key_ref.at[part], key_sem.at[g])
        )
        value_copies.append(
            pltpu.make_async_copy(value_hbm.at[part], value_ref.at[part], value_sem.at[g])
        )
    for copy in fetched[:3]:
        copy.start()
    for g in range(count):
        key_copies[g].start()
        value_copies[g].start()
    for copy in fetched[3:]:
        copy.start()

    fetched[0].wait()
    fetched[1].wait()
    widened = tokens_ref[...].astype(jnp.float32)
    factor = lax.rsqrt(jnp.mean(widened * widened, axis=-1, keepdims=True) + norm_epsilon)
    normed = (widened * factor * gain_ref[...]).astype(jnp.bfloat16)
    fetched[2].wait()
    queries = dot(normed, wq_ref[...]).astype(jnp.bfloat16)

    total = seqs * heads
    spread = jnp.zeros((total, HEAD), jnp.float32)
    r0, c0 = iota((total, seqs), 0), iota((total, seqs), 1)
    for h in range(heads):
        pick = (r0 == c0 * heads + h).astype(jnp.bfloat16)
        spread = spread + dot(pick, queries[:, h * HEAD : (h + 1) * HEAD])
    tiled = jnp.concatenate([spread.astype(jnp.bfloat16)] * group, axis=1)
    r1, c1 = iota((total, depth), 0), iota((total, depth), 1)
    own = (r1 // heads) % group == c1 // HEAD
    stacked = jnp.where(own, tiled, jnp.zeros_like(tiled))

    block = min(256, span)
    blocks = span // block
    tri = (iota((block, block), 0) >= iota((block, block), 1)).astype(jnp.bfloat16)
    row_id = iota((rows, 1), 0)
    bias_col = jnp.zeros((rows, 1), jnp.float32)
    for h in range(heads):
        bias_col = jnp.where(row_id % heads == h, bias[h], bias_col)
    place = iota((rows, span), 1)

    pieces = []
    for g in range(count):
        key_copies[g].wait()
        scores = dot(stacked[g * rows : (g + 1) * rows], key_ref[pl.ds(g * depth, depth), :])
        scores = scores * HEAD ** (-0.5) + bias_col
        length = jnp.zeros((rows, 1), jnp.int32)
        for j in range(group):
            length = jnp.where(row_id // heads == j, lengths[g * group + j], length)
        inside = place < length
        fall = -(jnp.maximum(scores, 0.0) + jnp.log1p(jnp.exp(-jnp.abs(scores))))
        fall = jnp.where(inside, fall, 0.0)
        high = fall.astype(jnp.bfloat16)
        low = (fall - high.astype(jnp.float32)).astype(jnp.bfloat16)
        cuts = [slice(b * block, (b + 1) * block) for b in range(blocks)]
        both = jnp.concatenate([high[:, c] for c in cuts] + [low[:, c] for c in cuts], axis=0)
        sums = dot(both, tri)
        later = jnp.zeros((rows, 1), jnp.float32)
        after = [None] * blocks
        for b in reversed(range(blocks)):
            within = (
                sums[b * rows : (b + 1) * rows]
                + sums[(blocks + b) * rows : (blocks + b + 1) * rows]
            )
            after[b] = within + later
            later = later + within[:, :1]
        weights = jnp.where(
            inside, jnp.exp(scores + jnp.concatenate(after, axis=1)), 0.0
        ).astype(jnp.bfloat16)
        value_copies[g].wait()
        pieces.append(dot_last(weights, value_ref[pl.ds(g * depth, depth), :]))
    mixed = jnp.where(own, jnp.concatenate(pieces, axis=0), 0.0)
    folded = mixed[:, :HEAD]
    for j in range(1, group):
        folded = folded + mixed[:, j * HEAD : (j + 1) * HEAD]
    folded = folded.astype(jnp.bfloat16)
    r2, c2 = iota((seqs, total), 0), iota((seqs, total), 1)
    attended = jnp.concatenate(
        [dot((c2 == r2 * heads + h).astype(jnp.bfloat16), folded) for h in range(heads)], axis=1
    ).astype(jnp.bfloat16)
    for copy in fetched[3:]:
        copy.wait()
    part_ref[...] = dot(attended, wo_ref[...]).astype(jnp.bfloat16)
    new_key_ref[...] = dot_last(normed, wk_ref[...]).astype(jnp.bfloat16)
    new_value_ref[...] = dot_last(normed, wv_ref[...]).astype(jnp.bfloat16)


def attend(tokens, gain, wq, wk, wv, bias, keys, values, lengths, wo):
    seqs, width = tokens.shape
    head_cols = wq.shape[1]
    kv_cols = wk.shape[1]
    assert kv_cols == HEAD
    span = keys.shape[2]
    group = 256 // HEAD
    while seqs % group:
        group //= 2
    hbm = pl.BlockSpec(memory_space=pltpu.HBM)
    smem = pl.BlockSpec(memory_space=pltpu.SMEM)
    vmem = pl.BlockSpec(memory_space=pltpu.VMEM)
    count = seqs // group
    bf = jnp.bfloat16
    return pl.pallas_call(
        functools.partial(attend_kernel, group),
        out_shape=(
            jax.ShapeDtypeStruct((seqs, width), bf),
            jax.ShapeDtypeStruct((seqs, kv_cols), bf),
            jax.ShapeDtypeStruct((seqs, kv_cols), bf),
        ),
        in_specs=[smem, smem] + [hbm] * 8,
        out_specs=(vmem, vmem, vmem),
        scratch_shapes=[
            pltpu.VMEM((seqs, width), bf),
            pltpu.VMEM((1, width), jnp.float32),
            pltpu.VMEM((width, head_cols), bf),
            pltpu.VMEM((kv_cols, width), bf),
            pltpu.VMEM((kv_cols, width), bf),
            pltpu.VMEM((head_cols, width), bf),
            pltpu.VMEM((seqs * kv_cols, span), bf),
            pltpu.VMEM((seqs * kv_cols, span), bf),
            pltpu.SemaphoreType.DMA((6,)),
            pltpu.SemaphoreType.DMA((count,)),
            pltpu.SemaphoreType.DMA((count,)),
        ],
        compiler_params=pltpu.CompilerParams(vmem_limit_bytes=24 * 1024 * 1024),
        cost_estimate=pl.CostEstimate(
            flops=4 * seqs * head_cols * span + 4 * seqs * width * head_cols,
            bytes_accessed=4 * seqs * kv_cols * span + 4 * width * head_cols,
            transcendentals=3 * seqs * head_cols // HEAD * span,
        ),
        name="attend",
    )(
        lengths,
        bias,
        tokens,
        gain.reshape(1, -1),
        wq,
        wk.T,
        wv.T,
        wo,
        keys.reshape(seqs * kv_cols, span),
        values.reshape(seqs * kv_cols, span),
    )


def rms_scale(inputs, gains):
    widened = inputs.astype(jnp.float32)
    factor = lax.rsqrt(jnp.mean(widened * widened, axis=-1, keepdims=True) + norm_epsilon)
    return (widened * factor * gains).astype(jnp.bfloat16)


def dispatch_matrix(block_routes, experts, capacity):
    flat_routes = block_routes.reshape(-1)
    onehot = (flat_routes[:, None] == jnp.arange(experts, dtype=jnp.int32)[None, :]).astype(
        jnp.float32
    )
    row_total = flat_routes.shape[0]
    row_ids = jnp.arange(row_total, dtype=jnp.int32)
    earlier = (row_ids[None, :] < row_ids[:, None]).astype(jnp.float32)
    before = jnp.dot(earlier, onehot, precision=lax.Precision.HIGHEST)
    slot_index = jnp.sum(before * onehot, axis=1).astype(jnp.int32)
    target = flat_routes * capacity + slot_index
    return jnp.arange(experts * capacity, dtype=jnp.int32)[:, None] == target[None, :]


def tp_total(part):
    size = lax.axis_size("tp")
    step = 1
    while step < size:
        swap = [(i, i ^ step) for i in range(size)]
        other = lax.ppermute(part, "tp", swap)
        part = part.astype(jnp.float32) + other.astype(jnp.float32)
        step *= 2
        if step < size:
            part = part.astype(jnp.bfloat16)
    return part


def body(
    tokens,
    attn_gain,
    w_query,
    w_key,
    w_value,
    attn_bias,
    key_cache,
    value_cache,
    lengths,
    w_out,
    ffn_gain,
    routes,
    route_weight,
    expert_gate,
    expert_up,
    expert_down,
):
    seq_count, model_width = tokens.shape
    partial_out, new_keys, new_values = attend(
        tokens,
        attn_gain,
        w_query,
        w_key,
        w_value,
        attn_bias,
        key_cache,
        value_cache,
        lengths,
        w_out,
    )
    attn_total = tp_total(partial_out)
    residual = (tokens.astype(jnp.float32) + attn_total).astype(jnp.bfloat16)
    normed_two = rms_scale(residual, ffn_gain)
    expert_count = lax.axis_size("ep")
    top_count = routes.shape[1]
    capacity = max(2, 2 * seq_count * top_count // expert_count)
    route_plan = dispatch_matrix(routes, expert_count, capacity).astype(jnp.bfloat16)
    repeated = jnp.repeat(normed_two, top_count, axis=0)
    outgoing = jnp.dot(route_plan, repeated, preferred_element_type=jnp.float32).astype(
        jnp.bfloat16
    )
    outgoing = outgoing.reshape(expert_count, capacity, model_width)
    gate_local = expert_gate[0]
    up_local = expert_up[0]
    down_local = expert_down[0]
    arrived = lax.all_to_all(outgoing, "ep", split_axis=0, concat_axis=0, tiled=True)
    sources, slot_count, row_width = arrived.shape
    row_block = arrived.reshape(sources * slot_count, row_width)
    gate_act = jnp.dot(row_block, gate_local, preferred_element_type=jnp.float32)
    lifted = jnp.dot(row_block, up_local, preferred_element_type=jnp.float32)
    hidden = (jax.nn.silu(gate_act) * lifted).astype(jnp.bfloat16)
    partial_value = jnp.dot(hidden, down_local, preferred_element_type=jnp.float32)
    returned = lax.all_to_all(
        partial_value.astype(jnp.bfloat16).reshape(sources, slot_count, row_width),
        "ep",
        split_axis=0,
        concat_axis=0,
        tiled=True,
    )
    flat_back = returned.reshape(expert_count * capacity, row_width)
    picked = jnp.dot(route_plan.T, flat_back, preferred_element_type=jnp.float32)
    picked = picked.reshape(seq_count, top_count, row_width)
    moe_part = jnp.sum(picked * route_weight[:, :, None], axis=1).astype(jnp.bfloat16)
    mixed_rows = (residual.astype(jnp.float32) + tp_total(moe_part)).astype(jnp.bfloat16)
    return (mixed_rows, new_keys, new_values)


def solution(mesh):
    return jax.shard_map(
        body,
        mesh=mesh,
        in_specs=(
            P("ep", None),
            P(),
            P(None, "tp"),
            P(None, "tp"),
            P(None, "tp"),
            P("tp"),
            P("ep", "tp", None),
            P("ep", "tp", None),
            P("ep"),
            P("tp", None),
            P(),
            P("ep", None),
            P("ep", None),
            P("ep", None, "tp"),
            P("ep", None, "tp"),
            P("ep", "tp", None),
        ),
        out_specs=(P("ep", None), P("ep", "tp"), P("ep", "tp")),
        check_vma=False,
    )
```

```python
import functools

import jax
import jax.numpy as jnp
from jax import lax
from jax.experimental import pallas as pl
from jax.experimental.pallas import tpu as pltpu
from jax.sharding import PartitionSpec as P

HEAD = 64
norm_epsilon = 1e-06

LAST = (((1,), (1,)), ((), ()))


def iota(shape, axis):
    return lax.broadcasted_iota(jnp.int32, shape, axis)


def dot(a, b):
    return jnp.dot(a, b, preferred_element_type=jnp.float32)


def dot_last(a, b):
    return lax.dot_general(a, b, LAST, preferred_element_type=jnp.float32)


def plan_rows(experts, capacity, routes, shares):
    top, seqs = routes.shape
    rows = slots_of(capacity)
    owner = iota((experts, seqs), 0)
    hits = [(owner == routes[k : k + 1, :]).astype(jnp.float32) for k in range(top)]
    any_hit = sum(hits[1:], hits[0])
    earlier = (iota((seqs, seqs), 0) < iota((seqs, seqs), 1)).astype(jnp.bfloat16)
    before = dot(any_hit.astype(jnp.bfloat16), earlier)
    eye = (iota((seqs, seqs), 0) == iota((seqs, seqs), 1)).astype(jnp.bfloat16)
    targets = []
    high_mix = jnp.zeros((experts, 128), jnp.float32)
    low_mix = jnp.zeros((experts, 128), jnp.float32)
    for k in range(top):
        slot = jnp.sum(hits[k] * before, axis=0, keepdims=True)
        targets.append(routes[k : k + 1, :].astype(jnp.float32) * rows + slot)
        spread = jnp.broadcast_to(slot, (8, seqs)).astype(jnp.bfloat16)
        column = dot_last(eye, spread)[:, :1].astype(jnp.int32)
        at = (iota((seqs, 128), 1) == column).astype(jnp.bfloat16)
        share = hits[k] * shares[k : k + 1, :]
        high = share.astype(jnp.bfloat16)
        low = (share - high.astype(jnp.float32)).astype(jnp.bfloat16)
        high_mix = high_mix + dot(high, at)
        low_mix = low_mix + dot(low, at)
    return targets, high_mix, low_mix


def plan_of(pack_ref, seqs, top, total):
    row = iota((total, seqs), 0)
    plan = jnp.zeros((total, seqs), jnp.float32)
    for k in range(top):
        target = pack_ref[seqs + k : seqs + k + 1, :seqs].astype(jnp.int32)
        plan = plan + (row == target).astype(jnp.float32)
    return plan.astype(jnp.bfloat16)


def slots_of(capacity):
    return -(-(capacity + 2) // 16) * 16


def attend_kernel(
    group,
    experts,
    capacity,
    lengths,
    bias,
    tokens_hbm,
    gain_hbm,
    wq_hbm,
    wk_hbm,
    wv_hbm,
    wo_hbm,
    key_hbm,
    value_hbm,
    route_hbm,
    weight_hbm,
    pack_ref,
    send_ref,
    new_key_ref,
    new_value_ref,
    tokens_ref,
    gain_ref,
    wq_ref,
    wk_ref,
    wv_ref,
    wo_ref,
    key_ref,
    value_ref,
    route_ref,
    weight_ref,
    small_sem,
    key_sem,
    value_sem,
):
    seqs = tokens_ref.shape[0]
    span = key_ref.shape[1]
    heads = wq_ref.shape[1] // HEAD
    depth = group * HEAD
    rows = group * heads
    count = seqs // group
    order = (
        (tokens_hbm, tokens_ref),
        (gain_hbm, gain_ref),
        (wq_hbm, wq_ref),
        (route_hbm, route_ref),
        (weight_hbm, weight_ref),
        (wo_hbm, wo_ref),
        (wk_hbm, wk_ref),
        (wv_hbm, wv_ref),
    )
    fetched = [
        pltpu.make_async_copy(src, dst, small_sem.at[i]) for i, (src, dst) in enumerate(order)
    ]
    key_copies, value_copies = [], []
    for g in range(count):
        part = pl.ds(g * depth, depth)
        key_copies.append(
            pltpu.make_async_copy(key_hbm.at[part], key_ref.at[part], key_sem.at[g])
        )
        value_copies.append(
            pltpu.make_async_copy(value_hbm.at[part], value_ref.at[part], value_sem.at[g])
        )
    for copy in fetched[:5]:
        copy.start()
    for copy in key_copies:
        copy.start()
    for copy in value_copies:
        copy.start()
    for copy in fetched[5:]:
        copy.start()

    fetched[0].wait()
    fetched[1].wait()
    widened = tokens_ref[...].astype(jnp.float32)
    factor = lax.rsqrt(jnp.mean(widened * widened, axis=-1, keepdims=True) + norm_epsilon)
    normed = (widened * factor * gain_ref[...]).astype(jnp.bfloat16)
    for copy in fetched[2:5]:
        copy.wait()
    queries = dot(normed, wq_ref[...]).astype(jnp.bfloat16)

    total = seqs * heads
    spread = jnp.zeros((total, HEAD), jnp.float32)
    r0, c0 = iota((total, seqs), 0), iota((total, seqs), 1)
    for h in range(heads):
        pick = (r0 == c0 * heads + h).astype(jnp.bfloat16)
        spread = spread + dot(pick, queries[:, h * HEAD : (h + 1) * HEAD])
    tiled = jnp.concatenate([spread.astype(jnp.bfloat16)] * group, axis=1)
    r1, c1 = iota((total, depth), 0), iota((total, depth), 1)
    own = (r1 // heads) % group == c1 // HEAD
    stacked = jnp.where(own, tiled, jnp.zeros_like(tiled))

    block = min(256, span)
    blocks = span // block
    tri = (iota((block, block), 0) >= iota((block, block), 1)).astype(jnp.bfloat16)
    row_id = iota((rows, 1), 0)
    bias_col = jnp.zeros((rows, 1), jnp.float32)
    for h in range(heads):
        bias_col = jnp.where(row_id % heads == h, bias[h], bias_col)
    place = iota((rows, span), 1)

    inside, scored, sums, weights, pieces = {}, {}, {}, {}, {}
    cuts = [slice(b * block, (b + 1) * block) for b in range(blocks)]

    def score(g):
        scores = dot(stacked[g * rows : (g + 1) * rows], key_ref[pl.ds(g * depth, depth), :])
        scores = scores * HEAD ** (-0.5) + bias_col
        length = jnp.zeros((rows, 1), jnp.int32)
        for j in range(group):
            length = jnp.where(row_id // heads == j, lengths[g * group + j], length)
        inside[g] = place < length
        fall = jnp.maximum(scores, 0.0) + jnp.log(1.0 + jnp.exp(-jnp.abs(scores)))
        fall = jnp.where(inside[g], -fall, 0.0)
        high = fall.astype(jnp.bfloat16)
        low = (fall - high.astype(jnp.float32)).astype(jnp.bfloat16)
        both = jnp.concatenate([high[:, c] for c in cuts] + [low[:, c] for c in cuts], axis=0)
        scored[g] = scores
        sums[g] = dot(both, tri)

    def weigh(g):
        later = jnp.zeros((rows, 1), jnp.float32)
        after = [None] * blocks
        for b in reversed(range(blocks)):
            within = (
                sums[g][b * rows : (b + 1) * rows]
                + sums[g][(blocks + b) * rows : (blocks + b + 1) * rows]
            )
            after[b] = within + later
            later = later + within[:, :1]
        weights[g] = jnp.where(
            inside[g], jnp.exp(scored[g] + jnp.concatenate(after, axis=1)), 0.0
        ).astype(jnp.bfloat16)

    def read(g):
        pieces[g] = dot_last(weights[g], value_ref[pl.ds(g * depth, depth), :])

    for step in range(count + 1):
        if step < count:
            key_copies[step].wait()
            score(step)
        if step >= 1:
            weigh(step - 1)
    targets, high_mix, low_mix = plan_rows(experts, capacity, route_ref[...], weight_ref[...])
    pack_ref[seqs:, :] = jnp.zeros((pack_ref.shape[0] - seqs, pack_ref.shape[1]), jnp.float32)
    for k, target in enumerate(targets):
        pack_ref[seqs + k : seqs + k + 1, :seqs] = target
    base_row = seqs + 8
    pack_ref[base_row : base_row + experts, :128] = high_mix
    pack_ref[base_row + experts : base_row + 2 * experts, :128] = low_mix
    for g in range(count):
        value_copies[g].wait()
        read(g)
    mixed = jnp.where(own, jnp.concatenate([pieces[g] for g in range(count)], axis=0), 0.0)
    folded = mixed[:, :HEAD]
    for j in range(1, group):
        folded = folded + mixed[:, j * HEAD : (j + 1) * HEAD]
    folded = folded.astype(jnp.bfloat16)
    r2, c2 = iota((seqs, total), 0), iota((seqs, total), 1)
    attended = jnp.concatenate(
        [dot((c2 == r2 * heads + h).astype(jnp.bfloat16), folded) for h in range(heads)], axis=1
    ).astype(jnp.bfloat16)
    for copy in fetched[5:]:
        copy.wait()
    out = dot(attended, wo_ref[...])
    half = out.shape[1] // 2
    low_core = lax.axis_index("core") == 0
    first = lax.axis_index("x") == 0
    keep = jnp.where(low_core, out[:, :half], out[:, half:])
    base = jnp.where(low_core, widened[:, :half], widened[:, half:])
    pack_ref[:seqs, :] = keep + jnp.where(first, base, jnp.zeros_like(base))
    send_ref[...] = jnp.where(low_core, out[:, half:], out[:, :half]).astype(jnp.bfloat16)
    new_key_ref[...] = dot_last(normed, wk_ref[...]).astype(jnp.bfloat16)
    new_value_ref[...] = dot_last(normed, wv_ref[...]).astype(jnp.bfloat16)


def attend(
    experts, capacity, tokens, gain, wq, wk, wv, bias, keys, values, lengths, wo, routes, shares
):
    seqs, width = tokens.shape
    head_cols = wq.shape[1]
    kv_cols = wk.shape[1]
    assert kv_cols == HEAD
    span = keys.shape[2]
    top = routes.shape[1]
    group = 256 // HEAD
    while seqs % group:
        group //= 2
    hbm = pl.BlockSpec(memory_space=pltpu.HBM)
    smem = pl.BlockSpec(memory_space=pltpu.SMEM)
    vmem = pl.BlockSpec(memory_space=pltpu.VMEM)
    count = seqs // group
    bf = jnp.bfloat16
    return pl.pallas_call(
        functools.partial(attend_kernel, group, experts, capacity),
        out_shape=(
            jax.ShapeDtypeStruct((seqs + 8 + 2 * experts, width // 2), jnp.float32),
            jax.ShapeDtypeStruct((seqs, width // 2), bf),
            jax.ShapeDtypeStruct((seqs, kv_cols), bf),
            jax.ShapeDtypeStruct((seqs, kv_cols), bf),
        ),
        in_specs=[smem, smem] + [hbm] * 10,
        out_specs=(vmem,) * 4,
        scratch_shapes=[
            pltpu.VMEM((seqs, width), bf),
            pltpu.VMEM((1, width), jnp.float32),
            pltpu.VMEM((width, head_cols), bf),
            pltpu.VMEM((kv_cols, width), bf),
            pltpu.VMEM((kv_cols, width), bf),
            pltpu.VMEM((head_cols, width), bf),
            pltpu.VMEM((seqs * kv_cols, span), bf),
            pltpu.VMEM((seqs * kv_cols, span), bf),
            pltpu.VMEM((top, seqs), jnp.int32),
            pltpu.VMEM((top, seqs), jnp.float32),
            pltpu.SemaphoreType.DMA((8,)),
            pltpu.SemaphoreType.DMA((count,)),
            pltpu.SemaphoreType.DMA((count,)),
        ],
        compiler_params=pltpu.CompilerParams(vmem_limit_bytes=67043328),
        cost_estimate=pl.CostEstimate(
            flops=4 * seqs * head_cols * span + 4 * seqs * width * head_cols,
            bytes_accessed=4 * seqs * kv_cols * span + 4 * width * head_cols,
            transcendentals=3 * seqs * head_cols // HEAD * span,
        ),
        name="attend",
    )(
        lengths,
        bias,
        tokens,
        gain.reshape(1, -1),
        wq,
        wk.T,
        wv.T,
        wo,
        keys.reshape(seqs * kv_cols, span),
        values.reshape(seqs * kv_cols, span),
        routes.T,
        shares.T,
    )


def scatter_kernel(capacity, top, pack_ref, got_ref, out_ref):
    experts, copies, rows, half = out_ref.shape
    seqs = got_ref.shape[0]
    total = experts * rows
    summed = (pack_ref[:seqs, :] + got_ref[...].astype(jnp.float32)).astype(jnp.bfloat16)
    placed = dot(plan_of(pack_ref, seqs, top, total), summed)
    mixes = pack_ref[seqs + 8 : seqs + 8 + 2 * experts, :128].astype(jnp.bfloat16)
    row, col = iota((total, 2 * experts), 0), iota((total, 2 * experts), 1)
    same = row // rows == col % experts
    turn = row % rows == capacity + col // experts
    pick = jnp.logical_and(same, turn).astype(jnp.bfloat16)
    lead = placed[:, :128] + dot(pick, mixes) * (1.0 / copies)
    whole = jnp.concatenate([lead, placed[:, 128:]], axis=1).astype(jnp.bfloat16)
    whole = whole.reshape(experts, rows, half)
    for copy in range(copies):
        out_ref[:, copy] = whole


def expert_kernel(
    capacity, copies, mine_ref, theirs_ref, gain_ref, gate_ref, up_ref, down_ref, keep_ref, send_ref
):
    sources, rows, half = mine_ref.shape
    total = sources * rows
    low_core = lax.axis_index("core") == 0
    mine = mine_ref[...].reshape(total, half)
    theirs = theirs_ref[...].reshape(total, half)
    residual = jnp.concatenate(
        [jnp.where(low_core, mine, theirs), jnp.where(low_core, theirs, mine)], axis=1
    ).astype(jnp.float32)
    factor = lax.rsqrt(jnp.mean(residual * residual, axis=-1, keepdims=True) + norm_epsilon)
    normed = (residual * factor * gain_ref[...]).astype(jnp.bfloat16)
    gated = dot(normed, gate_ref[...])
    lifted = dot(normed, up_ref[...])
    hidden = (gated / (1.0 + jnp.exp(-gated)) * lifted).astype(jnp.bfloat16)
    out = dot(hidden, down_ref[...])
    lanes = 128
    lead = mine_ref[:, :, :lanes].astype(jnp.float32)
    share = lead[:, capacity : capacity + 1] + lead[:, capacity + 1 : capacity + 2]
    share = jnp.broadcast_to(share, lead.shape).reshape(total, lanes)
    at_slot = iota((total, lanes), 0) % rows == iota((total, lanes), 1)
    share = jnp.sum(jnp.where(at_slot, share, 0.0), axis=1, keepdims=True)
    own = jnp.where(low_core, out[:, :half], out[:, half:])
    other = jnp.where(low_core, out[:, half:], out[:, :half])
    keep_ref[...] = (own * share + mine.astype(jnp.float32) * (1.0 / copies)).reshape(keep_ref.shape)
    send_ref[...] = (other * share).astype(jnp.bfloat16).reshape(send_ref.shape)


def gather_kernel(top, pack_ref, back_ref, out_ref):
    experts, copies, rows, half = back_ref.shape
    plan = plan_of(pack_ref, out_ref.shape[0], top, experts * rows)
    out = jnp.zeros(out_ref.shape, jnp.float32)
    for copy in range(copies):
        block = back_ref[:, copy].reshape(experts * rows, half)
        out = out + lax.dot_general(
            plan, block, (((0,), (0,)), ((), ())), preferred_element_type=jnp.float32
        )
    out_ref[...] = out.astype(jnp.bfloat16)


def local_call(kernel, outs, args, name, limit=16, flops=0):
    vmem = pl.BlockSpec(memory_space=pltpu.VMEM)
    moved = sum(a.size * a.dtype.itemsize for a in args)
    return pl.pallas_call(
        kernel,
        out_shape=outs,
        in_specs=[vmem] * len(args),
        out_specs=jax.tree.map(lambda _: vmem, outs),
        compiler_params=pltpu.CompilerParams(vmem_limit_bytes=limit * 1024 * 1024),
        cost_estimate=pl.CostEstimate(flops=flops, bytes_accessed=moved, transcendentals=0),
        name=name,
    )(*args)


def swap_core(value):
    return lax.ppermute(value, "core", [(0, 1), (1, 0)])


def body(
    tokens,
    attn_gain,
    w_query,
    w_key,
    w_value,
    attn_bias,
    key_cache,
    value_cache,
    lengths,
    w_out,
    ffn_gain,
    routes,
    route_weight,
    expert_gate,
    expert_up,
    expert_down,
):
    seqs, width = tokens.shape
    half = width // 2
    top = routes.shape[1]
    experts = lax.axis_size("ep")
    copies = lax.axis_size("x")
    capacity = max(2, 2 * seqs * top // experts)
    rows = slots_of(capacity)
    bf = jnp.bfloat16
    pack, send, new_keys, new_values = attend(
        experts,
        capacity,
        tokens,
        attn_gain,
        w_query,
        w_key,
        w_value,
        attn_bias,
        key_cache,
        value_cache,
        lengths,
        w_out,
        routes,
        route_weight,
    )
    outgoing = local_call(
        functools.partial(scatter_kernel, capacity, top),
        jax.ShapeDtypeStruct((experts, copies, rows, half), bf),
        (pack, swap_core(send)),
        "scatter",
        flops=20_000_000_000,
    )
    arrived = lax.all_to_all(
        outgoing.reshape(experts * copies, rows, half), ("ep", "x"), 0, 0, tiled=True
    )
    arrived = arrived.reshape(experts, copies, rows, half).astype(jnp.float32)
    mine = jnp.sum(arrived, axis=1).astype(bf)
    theirs = swap_core(mine)
    hidden = expert_gate.shape[2]
    keep, send = local_call(
        functools.partial(expert_kernel, capacity, top * copies),
        (
            jax.ShapeDtypeStruct((experts, rows, half), jnp.float32),
            jax.ShapeDtypeStruct((experts, rows, half), bf),
        ),
        (
            mine,
            theirs,
            ffn_gain.reshape(1, -1),
            expert_gate[0],
            expert_up[0],
            expert_down[0],
        ),
        "experts",
        flops=6 * experts * rows * width * hidden,
    )
    part = (keep + swap_core(send).astype(jnp.float32)).astype(bf)
    part = jnp.broadcast_to(part[:, None], (experts, copies, rows, half))
    back = lax.all_to_all(
        part.reshape(experts * copies, rows, half), ("ep", "x"), 0, 0, tiled=True
    )
    mixed = local_call(
        functools.partial(gather_kernel, top),
        jax.ShapeDtypeStruct((seqs, half), bf),
        (pack, back.reshape(experts, copies, rows, half)),
        "gather",
    )
    other = swap_core(mixed)
    low_core = lax.axis_index("core") == 0
    mixed_rows = jnp.concatenate(
        [jnp.where(low_core, mixed, other), jnp.where(low_core, other, mixed)], axis=1
    )
    return (mixed_rows, new_keys, new_values)


def solution(mesh):
    experts, parts = mesh.devices.shape
    split = jax.sharding.Mesh(
        mesh.devices.reshape(experts, parts // 2, 2), ("ep", "x", "core")
    )
    tp = ("x", "core")
    return jax.shard_map(
        body,
        mesh=split,
        in_specs=(
            P("ep", None),
            P(),
            P(None, tp),
            P(None, tp),
            P(None, tp),
            P(tp),
            P("ep", tp, None),
            P("ep", tp, None),
            P("ep"),
            P(tp, None),
            P(),
            P("ep", None),
            P("ep", None),
            P("ep", None, tp),
            P("ep", None, tp),
            P("ep", tp, None),
        ),
        out_specs=(P("ep", None), P("ep", tp), P("ep", tp)),
        check_vma=False,
    )
```

```python
import functools

import jax
import jax.numpy as jnp
from jax import lax
from jax.experimental import pallas as pl
from jax.experimental.pallas import tpu as pltpu
from jax.sharding import PartitionSpec as P

HEAD = 64
norm_epsilon = 1e-06

LAST = (((1,), (1,)), ((), ()))


def iota(shape, axis):
    return lax.broadcasted_iota(jnp.int32, shape, axis)


def dot(a, b):
    return jnp.dot(a, b, preferred_element_type=jnp.float32)


def dot_last(a, b):
    return lax.dot_general(a, b, LAST, preferred_element_type=jnp.float32)


def plan_rows(experts, capacity, routes, shares):
    top, seqs = routes.shape
    rows = slots_of(capacity)
    owner = iota((experts, seqs), 0)
    hits = [(owner == routes[k : k + 1, :]).astype(jnp.float32) for k in range(top)]
    any_hit = sum(hits[1:], hits[0])
    earlier = (iota((seqs, seqs), 0) < iota((seqs, seqs), 1)).astype(jnp.bfloat16)
    before = dot(any_hit.astype(jnp.bfloat16), earlier)
    eye = (iota((seqs, seqs), 0) == iota((seqs, seqs), 1)).astype(jnp.bfloat16)
    targets = []
    high_mix = jnp.zeros((experts, 128), jnp.float32)
    low_mix = jnp.zeros((experts, 128), jnp.float32)
    for k in range(top):
        slot = jnp.sum(hits[k] * before, axis=0, keepdims=True)
        targets.append(routes[k : k + 1, :].astype(jnp.float32) * rows + slot)
        spread = jnp.broadcast_to(slot, (8, seqs)).astype(jnp.bfloat16)
        column = dot_last(eye, spread)[:, :1].astype(jnp.int32)
        at = (iota((seqs, 128), 1) == column).astype(jnp.bfloat16)
        share = hits[k] * shares[k : k + 1, :]
        high = share.astype(jnp.bfloat16)
        low = (share - high.astype(jnp.float32)).astype(jnp.bfloat16)
        high_mix = high_mix + dot(high, at)
        low_mix = low_mix + dot(low, at)
    return targets, high_mix, low_mix


def plan_of(pack_ref, seqs, top, total):
    row = iota((total, seqs), 0)
    plan = jnp.zeros((total, seqs), jnp.float32)
    for k in range(top):
        target = pack_ref[seqs + k : seqs + k + 1, :seqs].astype(jnp.int32)
        plan = plan + (row == target).astype(jnp.float32)
    return plan.astype(jnp.bfloat16)


def slots_of(capacity):
    return -(-(capacity + 2) // 16) * 16


def attend_kernel(
    group,
    experts,
    capacity,
    lengths_hbm,
    bias_hbm,
    tokens_hbm,
    gain_hbm,
    wq_hbm,
    wk_hbm,
    wv_hbm,
    wo_hbm,
    key_hbm,
    value_hbm,
    route_hbm,
    weight_hbm,
    pack_ref,
    send_ref,
    new_key_ref,
    new_value_ref,
    lengths,
    bias,
    tokens_ref,
    gain_ref,
    wq_ref,
    wk_ref,
    wv_ref,
    wo_ref,
    key_ref,
    value_ref,
    route_ref,
    weight_ref,
    small_sem,
    key_sem,
    value_sem,
):
    seqs = tokens_ref.shape[0]
    span = key_ref.shape[1]
    heads = wq_ref.shape[1] // HEAD
    depth = group * HEAD
    rows = group * heads
    count = seqs // group
    early = (
        (tokens_hbm, tokens_ref),
        (gain_hbm, gain_ref),
        (wq_hbm, wq_ref),
        (lengths_hbm, lengths),
        (bias_hbm, bias),
        (route_hbm, route_ref),
        (weight_hbm, weight_ref),
    )
    late = ((wk_hbm, wk_ref), (wv_hbm, wv_ref), (wo_hbm, wo_ref))
    copies = [
        pltpu.make_async_copy(src, dst, small_sem.at[i])
        for i, (src, dst) in enumerate(early + late)
    ]
    fetched, last = copies[: len(early)], copies[len(early) :]

    def chunk(src, dst, sem, g):
        part = pl.ds(g * depth, depth)
        return pltpu.make_async_copy(src.at[part], dst.at[part], sem.at[g])

    stream = [chunk(key_hbm, key_ref, key_sem, g) for g in range(count)]
    stream += [chunk(value_hbm, value_ref, value_sem, g) for g in range(count)]
    stream.extend(last)
    started = [0]

    def start_to(limit):
        while started[0] < min(limit, len(stream)):
            stream[started[0]].start()
            started[0] += 1

    for copy in fetched:
        copy.start()
    start_to(max(1, count - 2))
    fetched[0].wait()
    fetched[1].wait()
    start_to(count)
    widened = tokens_ref[...].astype(jnp.float32)
    factor = lax.rsqrt(jnp.mean(widened * widened, axis=-1, keepdims=True) + norm_epsilon)
    normed = (widened * factor * gain_ref[...]).astype(jnp.bfloat16)
    for copy in fetched[2:]:
        copy.wait()
    start_to(len(stream))
    queries = dot(normed, wq_ref[...]).astype(jnp.bfloat16)

    total = seqs * heads
    spread = jnp.zeros((total, HEAD), jnp.float32)
    r0, c0 = iota((total, seqs), 0), iota((total, seqs), 1)
    for h in range(heads):
        pick = (r0 == c0 * heads + h).astype(jnp.bfloat16)
        spread = spread + dot(pick, queries[:, h * HEAD : (h + 1) * HEAD])
    tiled = jnp.concatenate([spread.astype(jnp.bfloat16)] * group, axis=1)
    r1, c1 = iota((total, depth), 0), iota((total, depth), 1)
    own = (r1 // heads) % group == c1 // HEAD
    stacked = jnp.where(own, tiled, jnp.zeros_like(tiled))

    block = min(256, span)
    blocks = span // block
    tri = (iota((block, block), 0) >= iota((block, block), 1)).astype(jnp.bfloat16)
    row_id = iota((rows, 1), 0)
    bias_col = jnp.zeros((rows, 1), jnp.float32)
    for h in range(heads):
        bias_col = jnp.where(row_id % heads == h, bias[h], bias_col)
    place = iota((rows, span), 1)

    inside, scored, sums, weights, pieces = {}, {}, {}, {}, {}
    cuts = [slice(b * block, (b + 1) * block) for b in range(blocks)]

    def score(g):
        scores = dot(stacked[g * rows : (g + 1) * rows], key_ref[pl.ds(g * depth, depth), :])
        scores = scores * HEAD ** (-0.5) + bias_col
        length = jnp.zeros((rows, 1), jnp.int32)
        for j in range(group):
            length = jnp.where(row_id // heads == j, lengths[g * group + j], length)
        inside[g] = place < length
        fall = jnp.maximum(scores, 0.0) + jnp.log(1.0 + jnp.exp(-jnp.abs(scores)))
        fall = jnp.where(inside[g], -fall, 0.0)
        high = fall.astype(jnp.bfloat16)
        low = (fall - high.astype(jnp.float32)).astype(jnp.bfloat16)
        both = jnp.concatenate([high[:, c] for c in cuts] + [low[:, c] for c in cuts], axis=0)
        scored[g] = scores
        sums[g] = dot(both, tri)

    def weigh(g):
        later = jnp.zeros((rows, 1), jnp.float32)
        after = [None] * blocks
        for b in reversed(range(blocks)):
            within = (
                sums[g][b * rows : (b + 1) * rows]
                + sums[g][(blocks + b) * rows : (blocks + b + 1) * rows]
            )
            after[b] = within + later
            later = later + within[:, :1]
        weights[g] = jnp.where(
            inside[g], jnp.exp(scored[g] + jnp.concatenate(after, axis=1)), 0.0
        ).astype(jnp.bfloat16)

    def read(g):
        pieces[g] = dot_last(weights[g], value_ref[pl.ds(g * depth, depth), :])

    targets, high_mix, low_mix = plan_rows(experts, capacity, route_ref[...], weight_ref[...])
    pack_ref[seqs:, :] = jnp.zeros((pack_ref.shape[0] - seqs, pack_ref.shape[1]), jnp.float32)
    for k, target in enumerate(targets):
        pack_ref[seqs + k : seqs + k + 1, :seqs] = target
    base_row = seqs + 8
    pack_ref[base_row : base_row + experts, :128] = high_mix
    pack_ref[base_row + experts : base_row + 2 * experts, :128] = low_mix
    for copy in stream[:count]:
        copy.wait()
    for g in range(count):
        score(g)
    for g in range(count):
        weigh(g)
    for copy in stream[count : 2 * count]:
        copy.wait()
    for g in range(count):
        read(g)
    mixed = jnp.where(own, jnp.concatenate([pieces[g] for g in range(count)], axis=0), 0.0)
    folded = mixed[:, :HEAD]
    for j in range(1, group):
        folded = folded + mixed[:, j * HEAD : (j + 1) * HEAD]
    folded = folded.astype(jnp.bfloat16)
    r2, c2 = iota((seqs, total), 0), iota((seqs, total), 1)
    attended = jnp.concatenate(
        [dot((c2 == r2 * heads + h).astype(jnp.bfloat16), folded) for h in range(heads)], axis=1
    ).astype(jnp.bfloat16)
    for copy in last:
        copy.wait()
    out = dot(attended, wo_ref[...])
    half = out.shape[1] // 2
    low_core = lax.axis_index("core") == 0
    first = lax.axis_index("x") == 0
    keep = jnp.where(low_core, out[:, :half], out[:, half:])
    base = jnp.where(low_core, widened[:, :half], widened[:, half:])
    pack_ref[:seqs, :] = keep + jnp.where(first, base, jnp.zeros_like(base))
    send_ref[...] = jnp.where(low_core, out[:, half:], out[:, :half]).astype(jnp.bfloat16)
    new_key_ref[...] = dot_last(normed, wk_ref[...]).astype(jnp.bfloat16)
    new_value_ref[...] = dot_last(normed, wv_ref[...]).astype(jnp.bfloat16)


def attend(
    experts, capacity, tokens, gain, wq, wk, wv, bias, keys, values, lengths, wo, routes, shares
):
    seqs, width = tokens.shape
    head_cols = wq.shape[1]
    kv_cols = wk.shape[1]
    assert kv_cols == HEAD
    span = keys.shape[2]
    top = routes.shape[1]
    group = 256 // HEAD
    while seqs % group:
        group //= 2
    hbm = pl.BlockSpec(memory_space=pltpu.HBM)
    vmem = pl.BlockSpec(memory_space=pltpu.VMEM)
    count = seqs // group
    bf = jnp.bfloat16
    return pl.pallas_call(
        functools.partial(attend_kernel, group, experts, capacity),
        out_shape=(
            jax.ShapeDtypeStruct((seqs + 8 + 2 * experts, width // 2), jnp.float32),
            jax.ShapeDtypeStruct((seqs, width // 2), bf),
            jax.ShapeDtypeStruct((seqs, kv_cols), bf),
            jax.ShapeDtypeStruct((seqs, kv_cols), bf),
        ),
        in_specs=[hbm] * 12,
        out_specs=(vmem,) * 4,
        scratch_shapes=[
            pltpu.SMEM((seqs,), jnp.int32),
            pltpu.SMEM((head_cols // HEAD,), jnp.float32),
            pltpu.VMEM((seqs, width), bf),
            pltpu.VMEM((1, width), jnp.float32),
            pltpu.VMEM((width, head_cols), bf),
            pltpu.VMEM((kv_cols, width), bf),
            pltpu.VMEM((kv_cols, width), bf),
            pltpu.VMEM((head_cols, width), bf),
            pltpu.VMEM((seqs * kv_cols, span), bf),
            pltpu.VMEM((seqs * kv_cols, span), bf),
            pltpu.VMEM((top, seqs), jnp.int32),
            pltpu.VMEM((top, seqs), jnp.float32),
            pltpu.SemaphoreType.DMA((10,)),
            pltpu.SemaphoreType.DMA((count,)),
            pltpu.SemaphoreType.DMA((count,)),
        ],
        compiler_params=pltpu.CompilerParams(vmem_limit_bytes=67043328),
        cost_estimate=pl.CostEstimate(
            flops=4 * seqs * head_cols * span + 4 * seqs * width * head_cols,
            bytes_accessed=4 * seqs * kv_cols * span + 4 * width * head_cols,
            transcendentals=3 * seqs * head_cols // HEAD * span,
        ),
        name="attend",
    )(
        lengths,
        bias,
        tokens,
        gain.reshape(1, -1),
        wq,
        wk.T,
        wv.T,
        wo,
        keys.reshape(seqs * kv_cols, span),
        values.reshape(seqs * kv_cols, span),
        routes.T,
        shares.T,
    )


def scatter_kernel(capacity, top, pack_ref, got_ref, out_ref):
    experts, copies, rows, half = out_ref.shape
    seqs = got_ref.shape[0]
    total = experts * rows
    summed = (pack_ref[:seqs, :] + got_ref[...].astype(jnp.float32)).astype(jnp.bfloat16)
    placed = dot(plan_of(pack_ref, seqs, top, total), summed)
    mixes = pack_ref[seqs + 8 : seqs + 8 + 2 * experts, :128].astype(jnp.bfloat16)
    row, col = iota((total, 2 * experts), 0), iota((total, 2 * experts), 1)
    same = row // rows == col % experts
    turn = row % rows == capacity + col // experts
    pick = jnp.logical_and(same, turn).astype(jnp.bfloat16)
    lead = placed[:, :128] + dot(pick, mixes) * (1.0 / copies)
    whole = jnp.concatenate([lead, placed[:, 128:]], axis=1).astype(jnp.bfloat16)
    whole = whole.reshape(experts, rows, half)
    for copy in range(copies):
        out_ref[:, copy] = whole


def expert_kernel(
    capacity, copies, mine_ref, theirs_ref, gain_ref, gate_ref, up_ref, down_ref, keep_ref, send_ref
):
    sources, rows, half = mine_ref.shape
    total = sources * rows
    low_core = lax.axis_index("core") == 0
    mine = mine_ref[...].reshape(total, half)
    theirs = theirs_ref[...].reshape(total, half)
    residual = jnp.concatenate(
        [jnp.where(low_core, mine, theirs), jnp.where(low_core, theirs, mine)], axis=1
    ).astype(jnp.float32)
    factor = lax.rsqrt(jnp.mean(residual * residual, axis=-1, keepdims=True) + norm_epsilon)
    normed = (residual * factor * gain_ref[...]).astype(jnp.bfloat16)
    gated = dot(normed, gate_ref[...])
    lifted = dot(normed, up_ref[...])
    hidden = (gated / (1.0 + jnp.exp(-gated)) * lifted).astype(jnp.bfloat16)
    out = dot(hidden, down_ref[...])
    lanes = 128
    lead = mine_ref[:, :, :lanes].astype(jnp.float32)
    share = lead[:, capacity : capacity + 1] + lead[:, capacity + 1 : capacity + 2]
    share = jnp.broadcast_to(share, lead.shape).reshape(total, lanes)
    at_slot = iota((total, lanes), 0) % rows == iota((total, lanes), 1)
    share = jnp.sum(jnp.where(at_slot, share, 0.0), axis=1, keepdims=True)
    own = jnp.where(low_core, out[:, :half], out[:, half:])
    other = jnp.where(low_core, out[:, half:], out[:, :half])
    keep_ref[...] = (own * share + mine.astype(jnp.float32) * (1.0 / copies)).reshape(keep_ref.shape)
    send_ref[...] = (other * share).astype(jnp.bfloat16).reshape(send_ref.shape)


def gather_kernel(top, pack_ref, back_ref, out_ref):
    experts, copies, rows, half = back_ref.shape
    plan = plan_of(pack_ref, out_ref.shape[0], top, experts * rows)
    out = jnp.zeros(out_ref.shape, jnp.float32)
    for copy in range(copies):
        block = back_ref[:, copy].reshape(experts * rows, half)
        out = out + lax.dot_general(
            plan, block, (((0,), (0,)), ((), ())), preferred_element_type=jnp.float32
        )
    out_ref[...] = out.astype(jnp.bfloat16)


def local_call(kernel, outs, args, name, limit=16, flops=0):
    vmem = pl.BlockSpec(memory_space=pltpu.VMEM)
    moved = sum(a.size * a.dtype.itemsize for a in args)
    return pl.pallas_call(
        kernel,
        out_shape=outs,
        in_specs=[vmem] * len(args),
        out_specs=jax.tree.map(lambda _: vmem, outs),
        compiler_params=pltpu.CompilerParams(vmem_limit_bytes=limit * 1024 * 1024),
        cost_estimate=pl.CostEstimate(flops=flops, bytes_accessed=moved, transcendentals=0),
        name=name,
    )(*args)


def swap_core(value):
    return lax.ppermute(value, "core", [(0, 1), (1, 0)])


def body(
    tokens,
    attn_gain,
    w_query,
    w_key,
    w_value,
    attn_bias,
    key_cache,
    value_cache,
    lengths,
    w_out,
    ffn_gain,
    routes,
    route_weight,
    expert_gate,
    expert_up,
    expert_down,
):
    seqs, width = tokens.shape
    half = width // 2
    top = routes.shape[1]
    experts = lax.axis_size("ep")
    copies = lax.axis_size("x")
    capacity = max(2, 2 * seqs * top // experts)
    rows = slots_of(capacity)
    bf = jnp.bfloat16
    pack, send, new_keys, new_values = attend(
        experts,
        capacity,
        tokens,
        attn_gain,
        w_query,
        w_key,
        w_value,
        attn_bias,
        key_cache,
        value_cache,
        lengths,
        w_out,
        routes,
        route_weight,
    )
    outgoing = local_call(
        functools.partial(scatter_kernel, capacity, top),
        jax.ShapeDtypeStruct((experts, copies, rows, half), bf),
        (pack, swap_core(send)),
        "scatter",
        flops=20_000_000_000,
    )
    arrived = lax.all_to_all(
        outgoing.reshape(experts * copies, rows, half), ("ep", "x"), 0, 0, tiled=True
    )
    arrived = arrived.reshape(experts, copies, rows, half).astype(jnp.float32)
    mine = jnp.sum(arrived, axis=1).astype(bf)
    theirs = swap_core(mine)
    hidden = expert_gate.shape[2]
    keep, send = local_call(
        functools.partial(expert_kernel, capacity, top * copies),
        (
            jax.ShapeDtypeStruct((experts, rows, half), jnp.float32),
            jax.ShapeDtypeStruct((experts, rows, half), bf),
        ),
        (
            mine,
            theirs,
            ffn_gain.reshape(1, -1),
            expert_gate[0],
            expert_up[0],
            expert_down[0],
        ),
        "experts",
        flops=6 * experts * rows * width * hidden,
    )
    part = (keep + swap_core(send).astype(jnp.float32)).astype(bf)
    part = jnp.broadcast_to(part[:, None], (experts, copies, rows, half))
    back = lax.all_to_all(
        part.reshape(experts * copies, rows, half), ("ep", "x"), 0, 0, tiled=True
    )
    mixed = local_call(
        functools.partial(gather_kernel, top),
        jax.ShapeDtypeStruct((seqs, half), bf),
        (pack, back.reshape(experts, copies, rows, half)),
        "gather",
    )
    other = swap_core(mixed)
    low_core = lax.axis_index("core") == 0
    mixed_rows = jnp.concatenate(
        [jnp.where(low_core, mixed, other), jnp.where(low_core, other, mixed)], axis=1
    )
    return (mixed_rows, new_keys, new_values)


def solution(mesh):
    experts, parts = mesh.devices.shape
    split = jax.sharding.Mesh(
        mesh.devices.reshape(experts, parts // 2, 2), ("ep", "x", "core")
    )
    tp = ("x", "core")
    return jax.shard_map(
        body,
        mesh=split,
        in_specs=(
            P("ep", None),
            P(),
            P(None, tp),
            P(None, tp),
            P(None, tp),
            P(tp),
            P("ep", tp, None),
            P("ep", tp, None),
            P("ep"),
            P(tp, None),
            P(),
            P("ep", None),
            P("ep", None),
            P("ep", None, tp),
            P("ep", None, tp),
            P("ep", tp, None),
        ),
        out_specs=(P("ep", None), P("ep", tp), P("ep", tp)),
        check_vma=False,
    )
```

```python
import functools

import jax
import jax.numpy as jnp
from jax import lax
from jax.experimental import pallas as pl
from jax.experimental.pallas import tpu as pltpu
from jax.sharding import PartitionSpec as P

HEAD = 64
norm_epsilon = 1e-06

LAST = (((1,), (1,)), ((), ()))


def iota(shape, axis):
    return lax.broadcasted_iota(jnp.int32, shape, axis)


def dot(a, b):
    return jnp.dot(a, b, preferred_element_type=jnp.float32)


def dot_last(a, b):
    return lax.dot_general(a, b, LAST, preferred_element_type=jnp.float32)


LANES = 128


def sizes_of(capacity, half):
    blocks = half // LANES
    back = -(-(capacity * blocks) // 8) * 8
    return blocks, back + 8, back


def plan_rows(experts, capacity, blocks, out_rows, back_rows, routes, shares):
    top, seqs = routes.shape
    owner = iota((experts, seqs), 0)
    hits = [(owner == routes[k : k + 1, :]).astype(jnp.float32) for k in range(top)]
    any_hit = sum(hits[1:], hits[0])
    earlier = (iota((seqs, seqs), 0) < iota((seqs, seqs), 1)).astype(jnp.bfloat16)
    before = dot(any_hit.astype(jnp.bfloat16), earlier)
    eye = (iota((seqs, seqs), 0) == iota((seqs, seqs), 1)).astype(jnp.bfloat16)
    targets = []
    high_mix = jnp.zeros((experts, LANES), jnp.float32)
    low_mix = jnp.zeros((experts, LANES), jnp.float32)
    for k in range(top):
        slot = jnp.sum(hits[k] * before, axis=0, keepdims=True)
        expert = routes[k : k + 1, :].astype(jnp.float32)
        for rows in (out_rows, back_rows):
            first = expert * rows + slot
            wide = jnp.concatenate([first + b * capacity for b in range(blocks)], axis=1)
            targets.append(wide)
        spread = jnp.broadcast_to(slot, (8, seqs)).astype(jnp.bfloat16)
        column = dot_last(eye, spread)[:, :1].astype(jnp.int32)
        at = (iota((seqs, LANES), 1) == column).astype(jnp.bfloat16)
        share = hits[k] * shares[k : k + 1, :]
        high = share.astype(jnp.bfloat16)
        low = (share - high.astype(jnp.float32)).astype(jnp.bfloat16)
        high_mix = high_mix + dot(high, at)
        low_mix = low_mix + dot(low, at)
    return targets, high_mix, low_mix


def plan_of(pack_ref, seqs, top, blocks, total, way):
    row = iota((total, blocks * seqs), 0)
    plan = jnp.zeros((total, blocks * seqs), jnp.float32)
    for k in range(top):
        at = seqs + 2 * k + way
        target = pack_ref[at : at + 1, : blocks * seqs].astype(jnp.int32)
        plan = plan + (row == target).astype(jnp.float32)
    return plan.astype(jnp.bfloat16)


def pick_kernel(experts, rows, back_rows, pick_ref):
    line, col = iota(pick_ref.shape, 0), iota((1, pick_ref.shape[1]), 1)
    want = (col % experts) * rows + back_rows + col // experts
    pick_ref[...] = (line == want).astype(jnp.float32).astype(jnp.bfloat16)


def attend_kernel(
    group,
    experts,
    capacity,
    lengths_hbm,
    bias_hbm,
    tokens_hbm,
    gain_hbm,
    wq_hbm,
    wk_hbm,
    wv_hbm,
    wo_hbm,
    key_hbm,
    value_hbm,
    route_hbm,
    weight_hbm,
    pack_ref,
    send_ref,
    new_key_ref,
    new_value_ref,
    lengths,
    bias,
    tokens_ref,
    gain_ref,
    wq_ref,
    wk_ref,
    wv_ref,
    wo_ref,
    key_ref,
    value_ref,
    route_ref,
    weight_ref,
    small_sem,
    key_sem,
    value_sem,
):
    seqs = tokens_ref.shape[0]
    span = key_ref.shape[1]
    heads = wq_ref.shape[1] // HEAD
    depth = group * HEAD
    rows = group * heads
    count = seqs // group
    early = (
        (tokens_hbm, tokens_ref),
        (gain_hbm, gain_ref),
        (wq_hbm, wq_ref),
        (lengths_hbm, lengths),
        (bias_hbm, bias),
        (route_hbm, route_ref),
        (weight_hbm, weight_ref),
    )
    late = ((wk_hbm, wk_ref), (wv_hbm, wv_ref), (wo_hbm, wo_ref))
    copies = [
        pltpu.make_async_copy(src, dst, small_sem.at[i])
        for i, (src, dst) in enumerate(early + late)
    ]
    fetched, last = copies[: len(early)], copies[len(early) :]

    def chunk(src, dst, sem, g):
        part = pl.ds(g * depth, depth)
        return pltpu.make_async_copy(src.at[part], dst.at[part], sem.at[g])

    stream = [chunk(key_hbm, key_ref, key_sem, g) for g in range(count)]
    stream += [chunk(value_hbm, value_ref, value_sem, g) for g in range(count)]
    stream.extend(last)
    started = [0]

    def start_to(limit):
        while started[0] < min(limit, len(stream)):
            stream[started[0]].start()
            started[0] += 1

    for copy in fetched:
        copy.start()
    start_to(max(1, count - 2))
    fetched[0].wait()
    fetched[1].wait()
    start_to(count)
    widened = tokens_ref[...].astype(jnp.float32)
    factor = lax.rsqrt(jnp.mean(widened * widened, axis=-1, keepdims=True) + norm_epsilon)
    normed = (widened * factor * gain_ref[...]).astype(jnp.bfloat16)
    for copy in fetched[2:]:
        copy.wait()
    start_to(len(stream))
    queries = dot(normed, wq_ref[...]).astype(jnp.bfloat16)

    total = seqs * heads
    spread = jnp.zeros((total, HEAD), jnp.float32)
    r0, c0 = iota((total, seqs), 0), iota((total, seqs), 1)
    for h in range(heads):
        pick = (r0 == c0 * heads + h).astype(jnp.bfloat16)
        spread = spread + dot(pick, queries[:, h * HEAD : (h + 1) * HEAD])
    tiled = jnp.concatenate([spread.astype(jnp.bfloat16)] * group, axis=1)
    r1, c1 = iota((total, depth), 0), iota((total, depth), 1)
    own = (r1 // heads) % group == c1 // HEAD
    stacked = jnp.where(own, tiled, jnp.zeros_like(tiled))

    block = min(256, span)
    blocks = span // block
    tri = (iota((block, block), 0) >= iota((block, block), 1)).astype(jnp.bfloat16)
    row_id = iota((rows, 1), 0)
    bias_col = jnp.zeros((rows, 1), jnp.float32)
    for h in range(heads):
        bias_col = jnp.where(row_id % heads == h, bias[h], bias_col)
    place = iota((rows, span), 1)

    inside, scored, sums, weights, pieces = {}, {}, {}, {}, {}
    cuts = [slice(b * block, (b + 1) * block) for b in range(blocks)]

    def score(g):
        scores = dot(stacked[g * rows : (g + 1) * rows], key_ref[pl.ds(g * depth, depth), :])
        scores = scores * HEAD ** (-0.5) + bias_col
        length = jnp.zeros((rows, 1), jnp.int32)
        for j in range(group):
            length = jnp.where(row_id // heads == j, lengths[g * group + j], length)
        inside[g] = place < length
        fall = jnp.maximum(scores, 0.0) + jnp.log(1.0 + jnp.exp(-jnp.abs(scores)))
        fall = jnp.where(inside[g], -fall, 0.0)
        high = fall.astype(jnp.bfloat16)
        low = (fall - high.astype(jnp.float32)).astype(jnp.bfloat16)
        both = jnp.concatenate([high[:, c] for c in cuts] + [low[:, c] for c in cuts], axis=0)
        scored[g] = scores
        sums[g] = dot(both, tri)

    def weigh(g):
        later = jnp.zeros((rows, 1), jnp.float32)
        after = [None] * blocks
        for b in reversed(range(blocks)):
            within = (
                sums[g][b * rows : (b + 1) * rows]
                + sums[g][(blocks + b) * rows : (blocks + b + 1) * rows]
            )
            after[b] = within + later
            later = later + within[:, :1]
        weights[g] = jnp.where(
            inside[g], jnp.exp(scored[g] + jnp.concatenate(after, axis=1)), 0.0
        ).astype(jnp.bfloat16)

    def read(g):
        pieces[g] = dot_last(weights[g], value_ref[pl.ds(g * depth, depth), :])

    blocks_out, out_rows, back_rows = sizes_of(capacity, pack_ref.shape[1])
    targets, high_mix, low_mix = plan_rows(
        experts, capacity, blocks_out, out_rows, back_rows, route_ref[...], weight_ref[...]
    )
    pack_ref[seqs:, :] = jnp.zeros((pack_ref.shape[0] - seqs, pack_ref.shape[1]), jnp.float32)
    for k, target in enumerate(targets):
        pack_ref[seqs + k : seqs + k + 1, : target.shape[1]] = target
    base_row = seqs + 8
    pack_ref[base_row : base_row + experts, :LANES] = high_mix
    pack_ref[base_row + experts : base_row + 2 * experts, :LANES] = low_mix
    for copy in stream[:count]:
        copy.wait()
    for g in range(count):
        score(g)
    for g in range(count):
        weigh(g)
    for copy in stream[count : 2 * count]:
        copy.wait()
    for g in range(count):
        read(g)
    mixed = jnp.where(own, jnp.concatenate([pieces[g] for g in range(count)], axis=0), 0.0)
    folded = mixed[:, :HEAD]
    for j in range(1, group):
        folded = folded + mixed[:, j * HEAD : (j + 1) * HEAD]
    folded = folded.astype(jnp.bfloat16)
    r2, c2 = iota((seqs, total), 0), iota((seqs, total), 1)
    attended = jnp.concatenate(
        [dot((c2 == r2 * heads + h).astype(jnp.bfloat16), folded) for h in range(heads)], axis=1
    ).astype(jnp.bfloat16)
    for copy in last:
        copy.wait()
    out = dot(attended, wo_ref[...])
    half = out.shape[1] // 2
    low_core = lax.axis_index("core") == 0
    first = lax.axis_index("x") == 0
    keep = jnp.where(low_core, out[:, :half], out[:, half:])
    base = jnp.where(low_core, widened[:, :half], widened[:, half:])
    pack_ref[:seqs, :] = keep + jnp.where(first, base, jnp.zeros_like(base))
    send_ref[...] = jnp.where(low_core, out[:, half:], out[:, :half]).astype(jnp.bfloat16)
    new_key_ref[...] = dot_last(normed, wk_ref[...]).astype(jnp.bfloat16)
    new_value_ref[...] = dot_last(normed, wv_ref[...]).astype(jnp.bfloat16)


def attend(
    experts, capacity, tokens, gain, wq, wk, wv, bias, keys, values, lengths, wo, routes, shares
):
    seqs, width = tokens.shape
    head_cols = wq.shape[1]
    kv_cols = wk.shape[1]
    assert kv_cols == HEAD
    span = keys.shape[2]
    top = routes.shape[1]
    group = 256 // HEAD
    while seqs % group:
        group //= 2
    hbm = pl.BlockSpec(memory_space=pltpu.HBM)
    vmem = pl.BlockSpec(memory_space=pltpu.VMEM)
    count = seqs // group
    bf = jnp.bfloat16
    return pl.pallas_call(
        functools.partial(attend_kernel, group, experts, capacity),
        out_shape=(
            jax.ShapeDtypeStruct((seqs + 8 + 2 * experts, width // 2), jnp.float32),
            jax.ShapeDtypeStruct((seqs, width // 2), bf),
            jax.ShapeDtypeStruct((seqs, kv_cols), bf),
            jax.ShapeDtypeStruct((seqs, kv_cols), bf),
        ),
        in_specs=[hbm] * 12,
        out_specs=(vmem,) * 4,
        scratch_shapes=[
            pltpu.SMEM((seqs,), jnp.int32),
            pltpu.SMEM((head_cols // HEAD,), jnp.float32),
            pltpu.VMEM((seqs, width), bf),
            pltpu.VMEM((1, width), jnp.float32),
            pltpu.VMEM((width, head_cols), bf),
            pltpu.VMEM((kv_cols, width), bf),
            pltpu.VMEM((kv_cols, width), bf),
            pltpu.VMEM((head_cols, width), bf),
            pltpu.VMEM((seqs * kv_cols, span), bf),
            pltpu.VMEM((seqs * kv_cols, span), bf),
            pltpu.VMEM((top, seqs), jnp.int32),
            pltpu.VMEM((top, seqs), jnp.float32),
            pltpu.SemaphoreType.DMA((10,)),
            pltpu.SemaphoreType.DMA((count,)),
            pltpu.SemaphoreType.DMA((count,)),
        ],
        compiler_params=pltpu.CompilerParams(vmem_limit_bytes=67043328),
        cost_estimate=pl.CostEstimate(
            flops=4 * seqs * head_cols * span + 4 * seqs * width * head_cols,
            bytes_accessed=4 * seqs * kv_cols * span + 4 * width * head_cols,
            transcendentals=3 * seqs * head_cols // HEAD * span,
        ),
        name="attend",
    )(
        lengths,
        bias,
        tokens,
        gain.reshape(1, -1),
        wq,
        wk.T,
        wv.T,
        wo,
        keys.reshape(seqs * kv_cols, span),
        values.reshape(seqs * kv_cols, span),
        routes.T,
        shares.T,
    )


def stacked_blocks(value, blocks):
    return jnp.concatenate([value[:, b * LANES : (b + 1) * LANES] for b in range(blocks)], axis=0)


def unstacked(value, blocks):
    rows = value.shape[0] // blocks
    return [value[b * rows : (b + 1) * rows] for b in range(blocks)]


def scatter_kernel(capacity, top, pack_ref, got_ref, pick_ref, out_ref):
    experts, copies, rows, lanes = out_ref.shape
    seqs, half = got_ref.shape
    blocks = half // lanes
    total = experts * rows
    summed = (pack_ref[:seqs, :] + got_ref[...].astype(jnp.float32)).astype(jnp.bfloat16)
    placed = dot(plan_of(pack_ref, seqs, top, blocks, total, 0), stacked_blocks(summed, blocks))
    mixes = pack_ref[seqs + 8 : seqs + 8 + 2 * experts, :lanes].astype(jnp.bfloat16)
    whole = (placed + dot(pick_ref[...], mixes) * (1.0 / copies)).astype(jnp.bfloat16)
    whole = whole.reshape(experts, rows, lanes)
    for copy in range(copies):
        out_ref[:, copy] = whole


def expert_kernel(
    capacity,
    copies,
    mine_ref,
    theirs_ref,
    gain_ref,
    gate_ref,
    up_ref,
    down_ref,
    keep_ref,
    send_ref,
    mine_rows,
    theirs_rows,
    left_ref,
    right_ref,
    keep_rows,
    send_rows,
):
    sources, _, lanes = mine_ref.shape
    back_rows = keep_ref.shape[1]
    half = left_ref.shape[2]
    pad = left_ref.shape[1]
    blocks = half // lanes
    total = sources * pad
    low_core = lax.axis_index("core") == 0
    mine_rows[...] = mine_ref[...].astype(jnp.float32)
    theirs_rows[...] = theirs_ref[...].astype(jnp.float32)
    if pad > capacity:
        rest = jnp.zeros((sources, pad - capacity, half), jnp.float32)
        left_ref[:, capacity:, :] = rest
        right_ref[:, capacity:, :] = rest
    for b in range(blocks):
        chunk = slice(b * capacity, (b + 1) * capacity)
        cols = slice(b * lanes, (b + 1) * lanes)
        a, c = mine_rows[:, chunk, :], theirs_rows[:, chunk, :]
        left_ref[:, :capacity, cols] = jnp.where(low_core, a, c)
        right_ref[:, :capacity, cols] = jnp.where(low_core, c, a)
    left = left_ref[...].reshape(total, half)
    right = right_ref[...].reshape(total, half)
    residual = jnp.concatenate([left, right], axis=1)
    factor = lax.rsqrt(jnp.mean(residual * residual, axis=-1, keepdims=True) + norm_epsilon)
    normed = (residual * factor * gain_ref[...]).astype(jnp.bfloat16)
    gated = dot(normed, gate_ref[...])
    lifted = dot(normed, up_ref[...])
    hidden = (gated / (1.0 + jnp.exp(-gated)) * lifted).astype(jnp.bfloat16)
    out = dot(hidden, down_ref[...])
    share = mine_rows[:, back_rows : back_rows + 1, :] + mine_rows[:, back_rows + 1 : back_rows + 2, :]
    share = jnp.broadcast_to(share, (sources, pad, lanes)).reshape(total, lanes)
    at_slot = iota((total, lanes), 1) == iota((total, lanes), 0) % pad
    share = jnp.sum(jnp.where(at_slot, share, 0.0), axis=1, keepdims=True)
    own = jnp.where(low_core, out[:, :half], out[:, half:]) * share
    own = own + jnp.where(low_core, left, right) * (1.0 / copies)
    other = jnp.where(low_core, out[:, half:], out[:, :half]) * share
    own = own.reshape(sources, pad, half)
    other = other.reshape(sources, pad, half)
    if back_rows > blocks * capacity:
        rest = jnp.zeros((sources, back_rows - blocks * capacity, lanes), jnp.float32)
        keep_rows[:, blocks * capacity :, :] = rest
        send_rows[:, blocks * capacity :, :] = rest
    for b in range(blocks):
        chunk = slice(b * capacity, (b + 1) * capacity)
        cols = slice(b * lanes, (b + 1) * lanes)
        keep_rows[:, chunk, :] = own[:, :capacity, cols]
        send_rows[:, chunk, :] = other[:, :capacity, cols]
    keep_ref[...] = keep_rows[...]
    send_ref[...] = send_rows[...].astype(jnp.bfloat16)


def gather_kernel(capacity, top, pack_ref, back_ref, out_ref):
    experts, copies, rows, lanes = back_ref.shape
    seqs, half = out_ref.shape
    blocks = half // lanes
    plan = plan_of(pack_ref, seqs, top, blocks, experts * rows, 1)
    out = jnp.zeros((blocks * seqs, lanes), jnp.float32)
    for copy in range(copies):
        block = back_ref[:, copy].reshape(experts * rows, lanes)
        out = out + lax.dot_general(
            plan, block, (((0,), (0,)), ((), ())), preferred_element_type=jnp.float32
        )
    out_ref[...] = jnp.concatenate(unstacked(out, blocks), axis=1).astype(jnp.bfloat16)


def local_call(kernel, outs, args, name, limit=16, flops=0, scratch=()):
    vmem = pl.BlockSpec(memory_space=pltpu.VMEM)
    moved = sum(a.size * a.dtype.itemsize for a in args)
    return pl.pallas_call(
        kernel,
        out_shape=outs,
        in_specs=[vmem] * len(args),
        out_specs=jax.tree.map(lambda _: vmem, outs),
        scratch_shapes=scratch,
        compiler_params=pltpu.CompilerParams(vmem_limit_bytes=limit * 1024 * 1024),
        cost_estimate=pl.CostEstimate(flops=flops, bytes_accessed=moved, transcendentals=0),
        name=name,
    )(*args)


def swap_core(value):
    return lax.ppermute(value, "core", [(0, 1), (1, 0)])


def body(
    tokens,
    attn_gain,
    w_query,
    w_key,
    w_value,
    attn_bias,
    key_cache,
    value_cache,
    lengths,
    w_out,
    ffn_gain,
    routes,
    route_weight,
    expert_gate,
    expert_up,
    expert_down,
):
    seqs, width = tokens.shape
    half = width // 2
    top = routes.shape[1]
    experts = lax.axis_size("ep")
    copies = lax.axis_size("x")
    capacity = max(2, 2 * seqs * top // experts)
    blocks, out_rows, back_rows = sizes_of(capacity, half)
    bf = jnp.bfloat16
    pack, send, new_keys, new_values = attend(
        experts,
        capacity,
        tokens,
        attn_gain,
        w_query,
        w_key,
        w_value,
        attn_bias,
        key_cache,
        value_cache,
        lengths,
        w_out,
        routes,
        route_weight,
    )
    pad = -(-capacity // 8) * 8
    f32 = jnp.float32
    pick = local_call(
        functools.partial(pick_kernel, experts, out_rows, back_rows),
        jax.ShapeDtypeStruct((experts * out_rows, 2 * experts), bf),
        (),
        "pick",
        flops=5_000_000_000,
    )
    outgoing = local_call(
        functools.partial(scatter_kernel, capacity, top),
        jax.ShapeDtypeStruct((experts, copies, out_rows, LANES), bf),
        (pack, swap_core(send), pick),
        "scatter",
        flops=20_000_000_000,
    )
    arrived = lax.all_to_all(
        outgoing.reshape(experts * copies, out_rows, LANES), ("ep", "x"), 0, 0, tiled=True
    )
    arrived = arrived.reshape(experts, copies, out_rows, LANES).astype(jnp.float32)
    mine = jnp.sum(arrived, axis=1).astype(bf)
    theirs = swap_core(mine)
    hidden = expert_gate.shape[2]
    keep, send = local_call(
        functools.partial(expert_kernel, capacity, top * copies),
        (
            jax.ShapeDtypeStruct((experts, back_rows, LANES), f32),
            jax.ShapeDtypeStruct((experts, back_rows, LANES), bf),
        ),
        (
            mine,
            theirs,
            ffn_gain.reshape(1, -1),
            expert_gate[0],
            expert_up[0],
            expert_down[0],
        ),
        "experts",
        flops=6 * experts * capacity * width * hidden,
        scratch=(
            pltpu.VMEM((experts, out_rows, LANES), f32),
            pltpu.VMEM((experts, out_rows, LANES), f32),
            pltpu.VMEM((experts, pad, half), f32),
            pltpu.VMEM((experts, pad, half), f32),
            pltpu.VMEM((experts, back_rows, LANES), f32),
            pltpu.VMEM((experts, back_rows, LANES), f32),
        ),
    )
    part = (keep + swap_core(send).astype(jnp.float32)).astype(bf)
    part = jnp.broadcast_to(part[:, None], (experts, copies, back_rows, LANES))
    back = lax.all_to_all(
        part.reshape(experts * copies, back_rows, LANES), ("ep", "x"), 0, 0, tiled=True
    )
    mixed = local_call(
        functools.partial(gather_kernel, capacity, top),
        jax.ShapeDtypeStruct((seqs, half), bf),
        (pack, back.reshape(experts, copies, back_rows, LANES)),
        "gather",
    )
    other = swap_core(mixed)
    low_core = lax.axis_index("core") == 0
    mixed_rows = jnp.concatenate(
        [jnp.where(low_core, mixed, other), jnp.where(low_core, other, mixed)], axis=1
    )
    return (mixed_rows, new_keys, new_values)


def solution(mesh):
    experts, parts = mesh.devices.shape
    split = jax.sharding.Mesh(
        mesh.devices.reshape(experts, parts // 2, 2), ("ep", "x", "core")
    )
    tp = ("x", "core")
    return jax.shard_map(
        body,
        mesh=split,
        in_specs=(
            P("ep", None),
            P(),
            P(None, tp),
            P(None, tp),
            P(None, tp),
            P(tp),
            P("ep", tp, None),
            P("ep", tp, None),
            P("ep"),
            P(tp, None),
            P(),
            P("ep", None),
            P("ep", None),
            P("ep", None, tp),
            P("ep", None, tp),
            P("ep", tp, None),
        ),
        out_specs=(P("ep", None), P("ep", tp), P("ep", tp)),
        check_vma=False,
    )
```

```python
import functools

import jax
import jax.numpy as jnp
from jax import lax
from jax.experimental import pallas as pl
from jax.experimental.pallas import tpu as pltpu
from jax.sharding import PartitionSpec as P

HEAD = 64
norm_epsilon = 1e-06

LAST = (((1,), (1,)), ((), ()))


def iota(shape, axis):
    return lax.broadcasted_iota(jnp.int32, shape, axis)


def dot(a, b):
    return jnp.dot(a, b, preferred_element_type=jnp.float32)


def dot_last(a, b):
    return lax.dot_general(a, b, LAST, preferred_element_type=jnp.float32)


LANES = 128


def sizes_of(capacity, half):
    blocks = half // LANES
    back = -(-(capacity * blocks) // 8) * 8
    return blocks, back + 8, back


def plan_rows(experts, capacity, blocks, out_rows, back_rows, routes, shares):
    top, seqs = routes.shape
    owner = iota((experts, seqs), 0)
    hits = [(owner == routes[k : k + 1, :]).astype(jnp.float32) for k in range(top)]
    any_hit = sum(hits[1:], hits[0])
    earlier = (iota((seqs, seqs), 0) < iota((seqs, seqs), 1)).astype(jnp.bfloat16)
    before = dot(any_hit.astype(jnp.bfloat16), earlier)
    eye = (iota((seqs, seqs), 0) == iota((seqs, seqs), 1)).astype(jnp.bfloat16)
    targets = []
    high_mix = jnp.zeros((experts, LANES), jnp.float32)
    low_mix = jnp.zeros((experts, LANES), jnp.float32)
    for k in range(top):
        slot = jnp.sum(hits[k] * before, axis=0, keepdims=True)
        expert = routes[k : k + 1, :].astype(jnp.float32)
        for rows in (out_rows, back_rows):
            first = expert * rows + slot
            wide = jnp.concatenate([first + b * capacity for b in range(blocks)], axis=1)
            targets.append(wide)
        spread = jnp.broadcast_to(slot, (8, seqs)).astype(jnp.bfloat16)
        column = dot_last(eye, spread)[:, :1].astype(jnp.int32)
        at = (iota((seqs, LANES), 1) == column).astype(jnp.bfloat16)
        share = hits[k] * shares[k : k + 1, :]
        high = share.astype(jnp.bfloat16)
        low = (share - high.astype(jnp.float32)).astype(jnp.bfloat16)
        high_mix = high_mix + dot(high, at)
        low_mix = low_mix + dot(low, at)
    return targets, high_mix, low_mix


def plan_of(pack_ref, seqs, top, blocks, total, way):
    row = iota((total, blocks * seqs), 0)
    plan = jnp.zeros((total, blocks * seqs), jnp.float32)
    for k in range(top):
        at = seqs + 2 * k + way
        target = pack_ref[at : at + 1, : blocks * seqs].astype(jnp.int32)
        plan = plan + (row == target).astype(jnp.float32)
    return plan.astype(jnp.bfloat16)


def pick_kernel(experts, rows, back_rows, pick_ref):
    line, col = iota(pick_ref.shape, 0), iota((1, pick_ref.shape[1]), 1)
    want = (col % experts) * rows + back_rows + col // experts
    pick_ref[...] = (line == want).astype(jnp.float32).astype(jnp.bfloat16)


def attend_kernel(
    group,
    experts,
    capacity,
    lengths_hbm,
    bias_hbm,
    tokens_hbm,
    gain_hbm,
    wq_hbm,
    wk_hbm,
    wv_hbm,
    wo_hbm,
    key_hbm,
    value_hbm,
    route_hbm,
    weight_hbm,
    pack_ref,
    send_ref,
    new_key_ref,
    new_value_ref,
    lengths,
    bias,
    tokens_ref,
    gain_ref,
    wq_ref,
    wk_ref,
    wv_ref,
    wo_ref,
    key_ref,
    value_ref,
    route_ref,
    weight_ref,
    small_sem,
    key_sem,
    value_sem,
):
    seqs = tokens_ref.shape[0]
    span = key_ref.shape[1]
    heads = wq_ref.shape[1] // HEAD
    depth = group * HEAD
    rows = group * heads
    count = seqs // group
    early = (
        (tokens_hbm, tokens_ref),
        (gain_hbm, gain_ref),
        (wq_hbm, wq_ref),
        (lengths_hbm, lengths),
        (bias_hbm, bias),
        (route_hbm, route_ref),
        (weight_hbm, weight_ref),
    )
    late = ((wk_hbm, wk_ref), (wv_hbm, wv_ref), (wo_hbm, wo_ref))
    copies = [
        pltpu.make_async_copy(src, dst, small_sem.at[i])
        for i, (src, dst) in enumerate(early + late)
    ]
    fetched, last = copies[: len(early)], copies[len(early) :]

    def chunk(src, dst, sem, g):
        part = pl.ds(g * depth, depth)
        return pltpu.make_async_copy(src.at[part], dst.at[part], sem.at[g])

    stream = [chunk(key_hbm, key_ref, key_sem, g) for g in range(count)]
    stream += last
    stream += [chunk(value_hbm, value_ref, value_sem, g) for g in range(count)]
    started = [0]

    def start_to(limit):
        while started[0] < min(limit, len(stream)):
            stream[started[0]].start()
            started[0] += 1

    for copy in fetched:
        copy.start()
    start_to(max(1, count - 2))
    fetched[0].wait()
    fetched[1].wait()
    start_to(count)
    widened = tokens_ref[...].astype(jnp.float32)
    factor = lax.rsqrt(jnp.mean(widened * widened, axis=-1, keepdims=True) + norm_epsilon)
    normed = (widened * factor * gain_ref[...]).astype(jnp.bfloat16)
    for copy in fetched[2:]:
        copy.wait()
    start_to(len(stream))
    queries = dot(normed, wq_ref[...]).astype(jnp.bfloat16)

    total = seqs * heads
    spread = jnp.zeros((total, HEAD), jnp.float32)
    r0, c0 = iota((total, seqs), 0), iota((total, seqs), 1)
    for h in range(heads):
        pick = (r0 == c0 * heads + h).astype(jnp.bfloat16)
        spread = spread + dot(pick, queries[:, h * HEAD : (h + 1) * HEAD])
    tiled = jnp.concatenate([spread.astype(jnp.bfloat16)] * group, axis=1)
    r1, c1 = iota((total, depth), 0), iota((total, depth), 1)
    own = (r1 // heads) % group == c1 // HEAD
    stacked = jnp.where(own, tiled, jnp.zeros_like(tiled))

    block = min(256, span)
    blocks = span // block
    tri = (iota((block, block), 0) >= iota((block, block), 1)).astype(jnp.bfloat16)
    row_id = iota((rows, 1), 0)
    bias_col = jnp.zeros((rows, 1), jnp.float32)
    for h in range(heads):
        bias_col = jnp.where(row_id % heads == h, bias[h], bias_col)
    place = iota((rows, span), 1)

    inside, scored, sums, weights, pieces = {}, {}, {}, {}, {}
    cuts = [slice(b * block, (b + 1) * block) for b in range(blocks)]

    def score(g):
        scores = dot(stacked[g * rows : (g + 1) * rows], key_ref[pl.ds(g * depth, depth), :])
        scores = scores * HEAD ** (-0.5) + bias_col
        length = jnp.zeros((rows, 1), jnp.int32)
        for j in range(group):
            length = jnp.where(row_id // heads == j, lengths[g * group + j], length)
        inside[g] = place < length
        fall = jnp.maximum(scores, 0.0) + jnp.log(1.0 + jnp.exp(-jnp.abs(scores)))
        fall = jnp.where(inside[g], -fall, 0.0)
        high = fall.astype(jnp.bfloat16)
        low = (fall - high.astype(jnp.float32)).astype(jnp.bfloat16)
        both = jnp.concatenate([high[:, c] for c in cuts] + [low[:, c] for c in cuts], axis=0)
        scored[g] = scores
        sums[g] = dot(both, tri)

    def weigh(g):
        later = jnp.zeros((rows, 1), jnp.float32)
        after = [None] * blocks
        for b in reversed(range(blocks)):
            within = (
                sums[g][b * rows : (b + 1) * rows]
                + sums[g][(blocks + b) * rows : (blocks + b + 1) * rows]
            )
            after[b] = within + later
            later = later + within[:, :1]
        weights[g] = jnp.where(
            inside[g], jnp.exp(scored[g] + jnp.concatenate(after, axis=1)), 0.0
        ).astype(jnp.bfloat16)

    def read(g):
        pieces[g] = dot_last(weights[g], value_ref[pl.ds(g * depth, depth), :])

    blocks_out, out_rows, back_rows = sizes_of(capacity, pack_ref.shape[1])
    targets, high_mix, low_mix = plan_rows(
        experts, capacity, blocks_out, out_rows, back_rows, route_ref[...], weight_ref[...]
    )
    pack_ref[seqs:, :] = jnp.zeros((pack_ref.shape[0] - seqs, pack_ref.shape[1]), jnp.float32)
    for k, target in enumerate(targets):
        pack_ref[seqs + k : seqs + k + 1, : target.shape[1]] = target
    base_row = seqs + 8
    pack_ref[base_row : base_row + experts, :LANES] = high_mix
    pack_ref[base_row + experts : base_row + 2 * experts, :LANES] = low_mix
    for copy in stream[:count]:
        copy.wait()
    for g in range(count):
        score(g)
    for g in range(count):
        weigh(g)
    for copy in last:
        copy.wait()
    new_key_ref[...] = dot_last(normed, wk_ref[...]).astype(jnp.bfloat16)
    new_value_ref[...] = dot_last(normed, wv_ref[...]).astype(jnp.bfloat16)
    for copy in stream[count + len(last) :]:
        copy.wait()
    for g in range(count):
        read(g)
    mixed = jnp.where(own, jnp.concatenate([pieces[g] for g in range(count)], axis=0), 0.0)
    folded = mixed[:, :HEAD]
    for j in range(1, group):
        folded = folded + mixed[:, j * HEAD : (j + 1) * HEAD]
    folded = folded.astype(jnp.bfloat16)
    r2, c2 = iota((seqs, total), 0), iota((seqs, total), 1)
    attended = jnp.concatenate(
        [dot((c2 == r2 * heads + h).astype(jnp.bfloat16), folded) for h in range(heads)], axis=1
    ).astype(jnp.bfloat16)
    out = dot(attended, wo_ref[...])
    half = out.shape[1] // 2
    low_core = lax.axis_index("core") == 0
    first = lax.axis_index("x") == 0
    keep = jnp.where(low_core, out[:, :half], out[:, half:])
    base = jnp.where(low_core, widened[:, :half], widened[:, half:])
    pack_ref[:seqs, :] = keep + jnp.where(first, base, jnp.zeros_like(base))
    send_ref[...] = jnp.where(low_core, out[:, half:], out[:, :half]).astype(jnp.bfloat16)


def attend(
    experts, capacity, tokens, gain, wq, wk, wv, bias, keys, values, lengths, wo, routes, shares
):
    seqs, width = tokens.shape
    head_cols = wq.shape[1]
    kv_cols = wk.shape[1]
    assert kv_cols == HEAD
    span = keys.shape[2]
    top = routes.shape[1]
    group = 256 // HEAD
    while seqs % group:
        group //= 2
    hbm = pl.BlockSpec(memory_space=pltpu.HBM)
    vmem = pl.BlockSpec(memory_space=pltpu.VMEM)
    count = seqs // group
    bf = jnp.bfloat16
    return pl.pallas_call(
        functools.partial(attend_kernel, group, experts, capacity),
        out_shape=(
            jax.ShapeDtypeStruct((seqs + 8 + 2 * experts, width // 2), jnp.float32),
            jax.ShapeDtypeStruct((seqs, width // 2), bf),
            jax.ShapeDtypeStruct((seqs, kv_cols), bf),
            jax.ShapeDtypeStruct((seqs, kv_cols), bf),
        ),
        in_specs=[hbm] * 12,
        out_specs=(vmem,) * 4,
        scratch_shapes=[
            pltpu.SMEM((seqs,), jnp.int32),
            pltpu.SMEM((head_cols // HEAD,), jnp.float32),
            pltpu.VMEM((seqs, width), bf),
            pltpu.VMEM((1, width), jnp.float32),
            pltpu.VMEM((width, head_cols), bf),
            pltpu.VMEM((kv_cols, width), bf),
            pltpu.VMEM((kv_cols, width), bf),
            pltpu.VMEM((head_cols, width), bf),
            pltpu.VMEM((seqs * kv_cols, span), bf),
            pltpu.VMEM((seqs * kv_cols, span), bf),
            pltpu.VMEM((top, seqs), jnp.int32),
            pltpu.VMEM((top, seqs), jnp.float32),
            pltpu.SemaphoreType.DMA((10,)),
            pltpu.SemaphoreType.DMA((count,)),
            pltpu.SemaphoreType.DMA((count,)),
        ],
        compiler_params=pltpu.CompilerParams(vmem_limit_bytes=67043328),
        cost_estimate=pl.CostEstimate(
            flops=4 * seqs * head_cols * span + 4 * seqs * width * head_cols,
            bytes_accessed=4 * seqs * kv_cols * span + 4 * width * head_cols,
            transcendentals=3 * seqs * head_cols // HEAD * span,
        ),
        name="attend",
    )(
        lengths,
        bias,
        tokens,
        gain.reshape(1, -1),
        wq,
        wk.T,
        wv.T,
        wo,
        keys.reshape(seqs * kv_cols, span),
        values.reshape(seqs * kv_cols, span),
        routes.T,
        shares.T,
    )


def stacked_blocks(value, blocks):
    return jnp.concatenate([value[:, b * LANES : (b + 1) * LANES] for b in range(blocks)], axis=0)


def unstacked(value, blocks):
    rows = value.shape[0] // blocks
    return [value[b * rows : (b + 1) * rows] for b in range(blocks)]


def scatter_kernel(capacity, top, pack_ref, got_ref, pick_ref, out_ref):
    copies, experts, rows, lanes = out_ref.shape
    seqs, half = got_ref.shape
    blocks = half // lanes
    total = experts * rows
    summed = (pack_ref[:seqs, :] + got_ref[...].astype(jnp.float32)).astype(jnp.bfloat16)
    placed = dot(plan_of(pack_ref, seqs, top, blocks, total, 0), stacked_blocks(summed, blocks))
    mixes = pack_ref[seqs + 8 : seqs + 8 + 2 * experts, :lanes].astype(jnp.bfloat16)
    whole = (placed + dot(pick_ref[...], mixes) * (1.0 / copies)).astype(jnp.bfloat16)
    whole = whole.reshape(experts, rows, lanes)
    for copy in range(copies):
        out_ref[copy] = whole


def expert_kernel(
    capacity,
    copies,
    mine_ref,
    theirs_ref,
    gain_ref,
    gate_ref,
    up_ref,
    down_ref,
    keep_ref,
    send_ref,
    mine_rows,
    theirs_rows,
    left_ref,
    right_ref,
    keep_rows,
    send_rows,
):
    sources, _, lanes = mine_ref.shape
    back_rows = keep_ref.shape[1]
    half = left_ref.shape[2]
    pad = left_ref.shape[1]
    blocks = half // lanes
    total = sources * pad
    low_core = lax.axis_index("core") == 0
    mine_rows[...] = mine_ref[...].astype(jnp.float32)
    theirs_rows[...] = theirs_ref[...].astype(jnp.float32)
    if pad > capacity:
        rest = jnp.zeros((sources, pad - capacity, half), jnp.float32)
        left_ref[:, capacity:, :] = rest
        right_ref[:, capacity:, :] = rest
    for b in range(blocks):
        chunk = slice(b * capacity, (b + 1) * capacity)
        cols = slice(b * lanes, (b + 1) * lanes)
        a, c = mine_rows[:, chunk, :], theirs_rows[:, chunk, :]
        left_ref[:, :capacity, cols] = jnp.where(low_core, a, c)
        right_ref[:, :capacity, cols] = jnp.where(low_core, c, a)
    left = left_ref[...].reshape(total, half)
    right = right_ref[...].reshape(total, half)
    residual = jnp.concatenate([left, right], axis=1)
    factor = lax.rsqrt(jnp.mean(residual * residual, axis=-1, keepdims=True) + norm_epsilon)
    normed = (residual * factor * gain_ref[...]).astype(jnp.bfloat16)
    gated = dot(normed, gate_ref[...])
    lifted = dot(normed, up_ref[...])
    hidden = (gated / (1.0 + jnp.exp(-gated)) * lifted).astype(jnp.bfloat16)
    out = dot(hidden, down_ref[...])
    share = mine_rows[:, back_rows : back_rows + 1, :] + mine_rows[:, back_rows + 1 : back_rows + 2, :]
    share = jnp.broadcast_to(share, (sources, pad, lanes)).reshape(total, lanes)
    at_slot = iota((total, lanes), 1) == iota((total, lanes), 0) % pad
    share = jnp.sum(jnp.where(at_slot, share, 0.0), axis=1, keepdims=True)
    own = jnp.where(low_core, out[:, :half], out[:, half:]) * share
    own = own + jnp.where(low_core, left, right) * (1.0 / copies)
    other = jnp.where(low_core, out[:, half:], out[:, :half]) * share
    own = own.reshape(sources, pad, half)
    other = other.reshape(sources, pad, half)
    if back_rows > blocks * capacity:
        rest = jnp.zeros((sources, back_rows - blocks * capacity, lanes), jnp.float32)
        keep_rows[:, blocks * capacity :, :] = rest
        send_rows[:, blocks * capacity :, :] = rest
    for b in range(blocks):
        chunk = slice(b * capacity, (b + 1) * capacity)
        cols = slice(b * lanes, (b + 1) * lanes)
        keep_rows[:, chunk, :] = own[:, :capacity, cols]
        send_rows[:, chunk, :] = other[:, :capacity, cols]
    keep_ref[...] = keep_rows[...]
    send_ref[...] = send_rows[...].astype(jnp.bfloat16)


def gather_kernel(capacity, top, pack_ref, back_ref, out_ref):
    copies, experts, rows, lanes = back_ref.shape
    seqs, half = out_ref.shape
    blocks = half // lanes
    plan = plan_of(pack_ref, seqs, top, blocks, experts * rows, 1)
    out = jnp.zeros((blocks * seqs, lanes), jnp.float32)
    for copy in range(copies):
        block = back_ref[copy].reshape(experts * rows, lanes)
        out = out + lax.dot_general(
            plan, block, (((0,), (0,)), ((), ())), preferred_element_type=jnp.float32
        )
    out_ref[...] = jnp.concatenate(unstacked(out, blocks), axis=1).astype(jnp.bfloat16)


def local_call(kernel, outs, args, name, limit=16, flops=0, scratch=()):
    vmem = pl.BlockSpec(memory_space=pltpu.VMEM)
    moved = sum(a.size * a.dtype.itemsize for a in args)
    return pl.pallas_call(
        kernel,
        out_shape=outs,
        in_specs=[vmem] * len(args),
        out_specs=jax.tree.map(lambda _: vmem, outs),
        scratch_shapes=scratch,
        compiler_params=pltpu.CompilerParams(vmem_limit_bytes=limit * 1024 * 1024),
        cost_estimate=pl.CostEstimate(flops=flops, bytes_accessed=moved, transcendentals=0),
        name=name,
    )(*args)


def swap_core(value):
    return lax.ppermute(value, "core", [(0, 1), (1, 0)])


def body(
    tokens,
    attn_gain,
    w_query,
    w_key,
    w_value,
    attn_bias,
    key_cache,
    value_cache,
    lengths,
    w_out,
    ffn_gain,
    routes,
    route_weight,
    expert_gate,
    expert_up,
    expert_down,
):
    seqs, width = tokens.shape
    half = width // 2
    top = routes.shape[1]
    experts = lax.axis_size("ep")
    copies = lax.axis_size("x")
    capacity = max(2, 2 * seqs * top // experts)
    blocks, out_rows, back_rows = sizes_of(capacity, half)
    bf = jnp.bfloat16
    pack, send, new_keys, new_values = attend(
        experts,
        capacity,
        tokens,
        attn_gain,
        w_query,
        w_key,
        w_value,
        attn_bias,
        key_cache,
        value_cache,
        lengths,
        w_out,
        routes,
        route_weight,
    )
    pad = -(-capacity // 8) * 8
    f32 = jnp.float32
    pick = local_call(
        functools.partial(pick_kernel, experts, out_rows, back_rows),
        jax.ShapeDtypeStruct((experts * out_rows, 2 * experts), bf),
        (),
        "pick",
        flops=5_000_000_000,
    )
    outgoing = local_call(
        functools.partial(scatter_kernel, capacity, top),
        jax.ShapeDtypeStruct((copies, experts, out_rows, LANES), bf),
        (pack, swap_core(send), pick),
        "scatter",
        flops=20_000_000_000,
    )
    arrived = lax.all_to_all(
        outgoing.reshape(copies * experts, out_rows, LANES), ("x", "ep"), 0, 0, tiled=True
    )
    arrived = arrived.reshape(copies, experts, out_rows, LANES).astype(f32)
    mine = sum([arrived[c] for c in range(1, copies)], arrived[0]).astype(bf)
    theirs = swap_core(mine)
    hidden = expert_gate.shape[2]
    keep, send = local_call(
        functools.partial(expert_kernel, capacity, top * copies),
        (
            jax.ShapeDtypeStruct((experts, back_rows, LANES), f32),
            jax.ShapeDtypeStruct((experts, back_rows, LANES), bf),
        ),
        (
            mine,
            theirs,
            ffn_gain.reshape(1, -1),
            expert_gate[0],
            expert_up[0],
            expert_down[0],
        ),
        "experts",
        flops=6 * experts * capacity * width * hidden,
        scratch=(
            pltpu.VMEM((experts, out_rows, LANES), f32),
            pltpu.VMEM((experts, out_rows, LANES), f32),
            pltpu.VMEM((experts, pad, half), f32),
            pltpu.VMEM((experts, pad, half), f32),
            pltpu.VMEM((experts, back_rows, LANES), f32),
            pltpu.VMEM((experts, back_rows, LANES), f32),
        ),
    )
    part = (keep + swap_core(send).astype(jnp.float32)).astype(bf)
    part = jnp.broadcast_to(part[None], (copies, experts, back_rows, LANES))
    back = lax.all_to_all(
        part.reshape(copies * experts, back_rows, LANES), ("x", "ep"), 0, 0, tiled=True
    )
    mixed = local_call(
        functools.partial(gather_kernel, capacity, top),
        jax.ShapeDtypeStruct((seqs, half), bf),
        (pack, back.reshape(copies, experts, back_rows, LANES)),
        "gather",
    )
    other = swap_core(mixed)
    low_core = lax.axis_index("core") == 0
    mixed_rows = jnp.concatenate(
        [jnp.where(low_core, mixed, other), jnp.where(low_core, other, mixed)], axis=1
    )
    return (mixed_rows, new_keys, new_values)


def solution(mesh):
    experts, parts = mesh.devices.shape
    split = jax.sharding.Mesh(
        mesh.devices.reshape(experts, parts // 2, 2), ("ep", "x", "core")
    )
    tp = ("x", "core")
    return jax.shard_map(
        body,
        mesh=split,
        in_specs=(
            P("ep", None),
            P(),
            P(None, tp),
            P(None, tp),
            P(None, tp),
            P(tp),
            P("ep", tp, None),
            P("ep", tp, None),
            P("ep"),
            P(tp, None),
            P(),
            P("ep", None),
            P("ep", None),
            P("ep", None, tp),
            P("ep", None, tp),
            P("ep", tp, None),
        ),
        out_specs=(P("ep", None), P("ep", tp), P("ep", tp)),
        check_vma=False,
    )
```

```python
import functools

import jax
import jax.numpy as jnp
from jax import lax
from jax.experimental import pallas as pl
from jax.experimental.pallas import tpu as pltpu
from jax.sharding import PartitionSpec as P

HEAD = 64
norm_epsilon = 1e-06

LAST = (((1,), (1,)), ((), ()))


def iota(shape, axis):
    return lax.broadcasted_iota(jnp.int32, shape, axis)


def dot(a, b):
    return jnp.dot(a, b, preferred_element_type=jnp.float32)


def dot_last(a, b):
    return lax.dot_general(a, b, LAST, preferred_element_type=jnp.float32)


LANES = 128


def sizes_of(capacity, half):
    blocks = half // LANES
    back = -(-(capacity * blocks) // 8) * 8
    return blocks, back + 8, back


def plan_rows(experts, capacity, blocks, out_rows, back_rows, routes, shares):
    top, seqs = routes.shape
    owner = iota((experts, seqs), 0)
    hits = [(owner == routes[k : k + 1, :]).astype(jnp.float32) for k in range(top)]
    any_hit = sum(hits[1:], hits[0])
    earlier = (iota((seqs, seqs), 0) < iota((seqs, seqs), 1)).astype(jnp.bfloat16)
    before = dot(any_hit.astype(jnp.bfloat16), earlier)
    eye = (iota((seqs, seqs), 0) == iota((seqs, seqs), 1)).astype(jnp.bfloat16)
    targets = []
    high_mix = jnp.zeros((experts, LANES), jnp.float32)
    low_mix = jnp.zeros((experts, LANES), jnp.float32)
    for k in range(top):
        slot = jnp.sum(hits[k] * before, axis=0, keepdims=True)
        expert = routes[k : k + 1, :].astype(jnp.float32)
        for rows in (out_rows, back_rows):
            first = expert * rows + slot
            wide = jnp.concatenate([first + b * capacity for b in range(blocks)], axis=1)
            targets.append(wide)
        spread = jnp.broadcast_to(slot, (8, seqs)).astype(jnp.bfloat16)
        column = dot_last(eye, spread)[:, :1].astype(jnp.int32)
        at = (iota((seqs, LANES), 1) == column).astype(jnp.bfloat16)
        share = hits[k] * shares[k : k + 1, :]
        high = share.astype(jnp.bfloat16)
        low = (share - high.astype(jnp.float32)).astype(jnp.bfloat16)
        high_mix = high_mix + dot(high, at)
        low_mix = low_mix + dot(low, at)
    return targets, high_mix, low_mix


def plan_of(pack_ref, seqs, top, blocks, total, way):
    row = iota((total, blocks * seqs), 0)
    plan = jnp.zeros((total, blocks * seqs), jnp.float32)
    for k in range(top):
        at = seqs + 2 * k + way
        target = pack_ref[at : at + 1, : blocks * seqs].astype(jnp.int32)
        plan = plan + (row == target).astype(jnp.float32)
    return plan.astype(jnp.bfloat16)


def pick_kernel(experts, rows, back_rows, pick_ref):
    line, col = iota(pick_ref.shape, 0), iota((1, pick_ref.shape[1]), 1)
    want = (col % experts) * rows + back_rows + col // experts
    pick_ref[...] = (line == want).astype(jnp.float32).astype(jnp.bfloat16)


def attend_kernel(
    group,
    experts,
    capacity,
    lengths_hbm,
    bias_hbm,
    tokens_hbm,
    gain_hbm,
    wq_hbm,
    wk_hbm,
    wv_hbm,
    wo_hbm,
    key_hbm,
    value_hbm,
    route_hbm,
    weight_hbm,
    pack_ref,
    send_ref,
    new_key_ref,
    new_value_ref,
    lengths,
    bias,
    tokens_ref,
    gain_ref,
    wq_ref,
    wk_ref,
    wv_ref,
    wo_ref,
    key_ref,
    value_ref,
    route_ref,
    weight_ref,
    small_sem,
    key_sem,
    value_sem,
):
    seqs = tokens_ref.shape[0]
    span = key_ref.shape[1]
    heads = wq_ref.shape[1] // HEAD
    depth = group * HEAD
    rows = group * heads
    count = seqs // group
    early = (
        (tokens_hbm, tokens_ref),
        (gain_hbm, gain_ref),
        (wq_hbm, wq_ref),
        (lengths_hbm, lengths),
        (bias_hbm, bias),
        (route_hbm, route_ref),
        (weight_hbm, weight_ref),
    )
    late = ((wk_hbm, wk_ref), (wv_hbm, wv_ref), (wo_hbm, wo_ref))
    copies = [
        pltpu.make_async_copy(src, dst, small_sem.at[i])
        for i, (src, dst) in enumerate(early + late)
    ]
    fetched, last = copies[: len(early)], copies[len(early) :]

    def chunk(src, dst, sem, g):
        part = pl.ds(g * depth, depth)
        return pltpu.make_async_copy(src.at[part], dst.at[part], sem.at[g])

    stream = [chunk(key_hbm, key_ref, key_sem, g) for g in range(count)]
    stream += last
    stream += [chunk(value_hbm, value_ref, value_sem, g) for g in range(count)]
    started = [0]

    def start_to(limit):
        while started[0] < min(limit, len(stream)):
            stream[started[0]].start()
            started[0] += 1

    for copy in fetched:
        copy.start()
    start_to(max(1, count - 2))
    fetched[0].wait()
    fetched[1].wait()
    start_to(count)
    widened = tokens_ref[...].astype(jnp.float32)
    factor = lax.rsqrt(jnp.mean(widened * widened, axis=-1, keepdims=True) + norm_epsilon)
    normed = (widened * factor * gain_ref[...]).astype(jnp.bfloat16)
    for copy in fetched[2:]:
        copy.wait()
    start_to(len(stream))
    queries = dot(normed, wq_ref[...]).astype(jnp.bfloat16)

    total = seqs * heads
    spread = jnp.zeros((total, HEAD), jnp.float32)
    r0, c0 = iota((total, seqs), 0), iota((total, seqs), 1)
    for h in range(heads):
        pick = (r0 == c0 * heads + h).astype(jnp.bfloat16)
        spread = spread + dot(pick, queries[:, h * HEAD : (h + 1) * HEAD])
    tiled = jnp.concatenate([spread.astype(jnp.bfloat16)] * group, axis=1)
    r1, c1 = iota((total, depth), 0), iota((total, depth), 1)
    own = (r1 // heads) % group == c1 // HEAD
    stacked = jnp.where(own, tiled, jnp.zeros_like(tiled))

    block = min(256, span)
    blocks = span // block
    tri = (iota((block, block), 0) >= iota((block, block), 1)).astype(jnp.bfloat16)
    row_id = iota((rows, 1), 0)
    bias_col = jnp.zeros((rows, 1), jnp.float32)
    for h in range(heads):
        bias_col = jnp.where(row_id % heads == h, bias[h], bias_col)
    place = iota((rows, span), 1)

    inside, scored, sums, weights, pieces = {}, {}, {}, {}, {}
    cuts = [slice(b * block, (b + 1) * block) for b in range(blocks)]

    def score(g):
        scores = dot(stacked[g * rows : (g + 1) * rows], key_ref[pl.ds(g * depth, depth), :])
        scores = scores * HEAD ** (-0.5) + bias_col
        length = jnp.zeros((rows, 1), jnp.int32)
        for j in range(group):
            length = jnp.where(row_id // heads == j, lengths[g * group + j], length)
        inside[g] = place < length
        fall = jnp.maximum(scores, 0.0) + jnp.log(1.0 + jnp.exp(-jnp.abs(scores)))
        fall = jnp.where(inside[g], -fall, 0.0)
        high = fall.astype(jnp.bfloat16)
        low = (fall - high.astype(jnp.float32)).astype(jnp.bfloat16)
        both = jnp.concatenate([high[:, c] for c in cuts] + [low[:, c] for c in cuts], axis=0)
        scored[g] = scores
        sums[g] = dot(both, tri)

    def weigh(g):
        later = jnp.zeros((rows, 1), jnp.float32)
        after = [None] * blocks
        for b in reversed(range(blocks)):
            within = (
                sums[g][b * rows : (b + 1) * rows]
                + sums[g][(blocks + b) * rows : (blocks + b + 1) * rows]
            )
            after[b] = within + later
            later = later + within[:, :1]
        weights[g] = jnp.where(
            inside[g], jnp.exp(scored[g] + jnp.concatenate(after, axis=1)), 0.0
        ).astype(jnp.bfloat16)

    def read(g):
        pieces[g] = dot_last(weights[g], value_ref[pl.ds(g * depth, depth), :])

    blocks_out, out_rows, back_rows = sizes_of(capacity, pack_ref.shape[1])
    targets, high_mix, low_mix = plan_rows(
        experts, capacity, blocks_out, out_rows, back_rows, route_ref[...], weight_ref[...]
    )
    pack_ref[seqs:, :] = jnp.zeros((pack_ref.shape[0] - seqs, pack_ref.shape[1]), jnp.float32)
    for k, target in enumerate(targets):
        pack_ref[seqs + k : seqs + k + 1, : target.shape[1]] = target
    base_row = seqs + 8
    pack_ref[base_row : base_row + experts, :LANES] = high_mix
    pack_ref[base_row + experts : base_row + 2 * experts, :LANES] = low_mix
    for copy in stream[:count]:
        copy.wait()
    for g in range(count):
        score(g)
    for g in range(count):
        weigh(g)
    for copy in last:
        copy.wait()
    new_key_ref[...] = dot_last(normed, wk_ref[...]).astype(jnp.bfloat16)
    new_value_ref[...] = dot_last(normed, wv_ref[...]).astype(jnp.bfloat16)
    for copy in stream[count + len(last) :]:
        copy.wait()
    for g in range(count):
        read(g)
    mixed = jnp.where(own, jnp.concatenate([pieces[g] for g in range(count)], axis=0), 0.0)
    folded = mixed[:, :HEAD]
    for j in range(1, group):
        folded = folded + mixed[:, j * HEAD : (j + 1) * HEAD]
    folded = folded.astype(jnp.bfloat16)
    r2, c2 = iota((seqs, total), 0), iota((seqs, total), 1)
    attended = jnp.concatenate(
        [dot((c2 == r2 * heads + h).astype(jnp.bfloat16), folded) for h in range(heads)], axis=1
    ).astype(jnp.bfloat16)
    out = dot(attended, wo_ref[...])
    half = out.shape[1] // 2
    low_core = lax.axis_index("core") == 0
    first = lax.axis_index("x") == 0
    keep = jnp.where(low_core, out[:, :half], out[:, half:])
    base = jnp.where(low_core, widened[:, :half], widened[:, half:])
    pack_ref[:seqs, :] = keep + jnp.where(first, base, jnp.zeros_like(base))
    send_ref[...] = jnp.where(low_core, out[:, half:], out[:, :half]).astype(jnp.bfloat16)


def attend(
    experts, capacity, tokens, gain, wq, wk, wv, bias, keys, values, lengths, wo, routes, shares
):
    seqs, width = tokens.shape
    head_cols = wq.shape[1]
    kv_cols = wk.shape[1]
    assert kv_cols == HEAD
    span = keys.shape[2]
    top = routes.shape[1]
    group = 256 // HEAD
    while seqs % group:
        group //= 2
    hbm = pl.BlockSpec(memory_space=pltpu.HBM)
    vmem = pl.BlockSpec(memory_space=pltpu.VMEM)
    count = seqs // group
    bf = jnp.bfloat16
    return pl.pallas_call(
        functools.partial(attend_kernel, group, experts, capacity),
        out_shape=(
            jax.ShapeDtypeStruct((seqs + 8 + 2 * experts, width // 2), jnp.float32),
            jax.ShapeDtypeStruct((seqs, width // 2), bf),
            jax.ShapeDtypeStruct((seqs, kv_cols), bf),
            jax.ShapeDtypeStruct((seqs, kv_cols), bf),
        ),
        in_specs=[hbm] * 12,
        out_specs=(vmem,) * 4,
        scratch_shapes=[
            pltpu.SMEM((seqs,), jnp.int32),
            pltpu.SMEM((head_cols // HEAD,), jnp.float32),
            pltpu.VMEM((seqs, width), bf),
            pltpu.VMEM((1, width), jnp.float32),
            pltpu.VMEM((width, head_cols), bf),
            pltpu.VMEM((kv_cols, width), bf),
            pltpu.VMEM((kv_cols, width), bf),
            pltpu.VMEM((head_cols, width), bf),
            pltpu.VMEM((seqs * kv_cols, span), bf),
            pltpu.VMEM((seqs * kv_cols, span), bf),
            pltpu.VMEM((top, seqs), jnp.int32),
            pltpu.VMEM((top, seqs), jnp.float32),
            pltpu.SemaphoreType.DMA((10,)),
            pltpu.SemaphoreType.DMA((count,)),
            pltpu.SemaphoreType.DMA((count,)),
        ],
        compiler_params=pltpu.CompilerParams(vmem_limit_bytes=67043328),
        cost_estimate=pl.CostEstimate(
            flops=4 * seqs * head_cols * span + 4 * seqs * width * head_cols,
            bytes_accessed=4 * seqs * kv_cols * span + 4 * width * head_cols,
            transcendentals=3 * seqs * head_cols // HEAD * span,
        ),
        name="attend",
    )(
        lengths,
        bias,
        tokens,
        gain.reshape(1, -1),
        wq,
        wk.T,
        wv.T,
        wo,
        keys.reshape(seqs * kv_cols, span),
        values.reshape(seqs * kv_cols, span),
        routes.T,
        shares.T,
    )


def stacked_blocks(value, blocks):
    return jnp.concatenate([value[:, b * LANES : (b + 1) * LANES] for b in range(blocks)], axis=0)


def unstacked(value, blocks):
    rows = value.shape[0] // blocks
    return [value[b * rows : (b + 1) * rows] for b in range(blocks)]


def scatter_kernel(capacity, top, pack_ref, got_ref, pick_ref, out_ref):
    copies, experts, rows, lanes = out_ref.shape
    seqs, half = got_ref.shape
    blocks = half // lanes
    total = experts * rows
    summed = (pack_ref[:seqs, :] + got_ref[...].astype(jnp.float32)).astype(jnp.bfloat16)
    placed = dot(plan_of(pack_ref, seqs, top, blocks, total, 0), stacked_blocks(summed, blocks))
    mixes = pack_ref[seqs + 8 : seqs + 8 + 2 * experts, :lanes].astype(jnp.bfloat16)
    whole = (placed + dot(pick_ref[...], mixes) * (1.0 / copies)).astype(jnp.bfloat16)
    whole = whole.reshape(experts, rows, lanes)
    for copy in range(copies):
        out_ref[copy] = whole


def add_kernel(arrived_ref, out_ref):
    whole = arrived_ref[0].astype(jnp.float32)
    for copy in range(1, arrived_ref.shape[0]):
        whole = whole + arrived_ref[copy].astype(jnp.float32)
    out_ref[...] = whole.astype(jnp.bfloat16)


def expert_kernel(
    capacity,
    copies,
    mine_ref,
    theirs_ref,
    gain_ref,
    gate_ref,
    up_ref,
    down_ref,
    keep_ref,
    send_ref,
    mine_rows,
    theirs_rows,
    left_ref,
    right_ref,
    keep_rows,
    send_rows,
):
    sources, _, lanes = mine_ref.shape
    back_rows = keep_ref.shape[1]
    half = left_ref.shape[2]
    pad = left_ref.shape[1]
    blocks = half // lanes
    total = sources * pad
    low_core = lax.axis_index("core") == 0
    mine_rows[...] = mine_ref[...].astype(jnp.float32)
    theirs_rows[...] = theirs_ref[...].astype(jnp.float32)
    if pad > capacity:
        rest = jnp.zeros((sources, pad - capacity, half), jnp.float32)
        left_ref[:, capacity:, :] = rest
        right_ref[:, capacity:, :] = rest
    for b in range(blocks):
        chunk = slice(b * capacity, (b + 1) * capacity)
        cols = slice(b * lanes, (b + 1) * lanes)
        a, c = mine_rows[:, chunk, :], theirs_rows[:, chunk, :]
        left_ref[:, :capacity, cols] = jnp.where(low_core, a, c)
        right_ref[:, :capacity, cols] = jnp.where(low_core, c, a)
    left = left_ref[...].reshape(total, half)
    right = right_ref[...].reshape(total, half)
    residual = jnp.concatenate([left, right], axis=1)
    factor = lax.rsqrt(jnp.mean(residual * residual, axis=-1, keepdims=True) + norm_epsilon)
    normed = (residual * factor * gain_ref[...]).astype(jnp.bfloat16)
    units = gate_ref.shape[1]
    pieces = []
    for start in range(0, units, 256):
        part = slice(start, min(start + 256, units))
        gated = dot(normed, gate_ref[:, part])
        lifted = dot(normed, up_ref[:, part])
        pieces.append((gated / (1.0 + jnp.exp(-gated)) * lifted).astype(jnp.bfloat16))
    out = dot(jnp.concatenate(pieces, axis=1), down_ref[...])
    share = mine_rows[:, back_rows : back_rows + 1, :] + mine_rows[:, back_rows + 1 : back_rows + 2, :]
    share = jnp.broadcast_to(share, (sources, pad, lanes)).reshape(total, lanes)
    at_slot = iota((total, lanes), 1) == iota((total, lanes), 0) % pad
    share = jnp.sum(jnp.where(at_slot, share, 0.0), axis=1, keepdims=True)
    own = jnp.where(low_core, out[:, :half], out[:, half:]) * share
    own = own + jnp.where(low_core, left, right) * (1.0 / copies)
    other = jnp.where(low_core, out[:, half:], out[:, :half]) * share
    own = own.reshape(sources, pad, half)
    other = other.reshape(sources, pad, half)
    if back_rows > blocks * capacity:
        rest = jnp.zeros((sources, back_rows - blocks * capacity, lanes), jnp.float32)
        keep_rows[:, blocks * capacity :, :] = rest
        send_rows[:, blocks * capacity :, :] = rest
    for b in range(blocks):
        chunk = slice(b * capacity, (b + 1) * capacity)
        cols = slice(b * lanes, (b + 1) * lanes)
        keep_rows[:, chunk, :] = own[:, :capacity, cols]
        send_rows[:, chunk, :] = other[:, :capacity, cols]
    keep_ref[...] = keep_rows[...]
    send_ref[...] = send_rows[...].astype(jnp.bfloat16)


def gather_kernel(capacity, top, pack_ref, back_ref, out_ref):
    copies, experts, rows, lanes = back_ref.shape
    seqs, half = out_ref.shape
    blocks = half // lanes
    plan = plan_of(pack_ref, seqs, top, blocks, experts * rows, 1)
    out = jnp.zeros((blocks * seqs, lanes), jnp.float32)
    for copy in range(copies):
        block = back_ref[copy].reshape(experts * rows, lanes)
        out = out + lax.dot_general(
            plan, block, (((0,), (0,)), ((), ())), preferred_element_type=jnp.float32
        )
    out_ref[...] = jnp.concatenate(unstacked(out, blocks), axis=1).astype(jnp.bfloat16)


def local_call(kernel, outs, args, name, limit=16, flops=0, scratch=()):
    vmem = pl.BlockSpec(memory_space=pltpu.VMEM)
    moved = sum(a.size * a.dtype.itemsize for a in args)
    return pl.pallas_call(
        kernel,
        out_shape=outs,
        in_specs=[vmem] * len(args),
        out_specs=jax.tree.map(lambda _: vmem, outs),
        scratch_shapes=scratch,
        compiler_params=pltpu.CompilerParams(vmem_limit_bytes=limit * 1024 * 1024),
        cost_estimate=pl.CostEstimate(flops=flops, bytes_accessed=moved, transcendentals=0),
        name=name,
    )(*args)


def swap_core(value):
    return lax.ppermute(value, "core", [(0, 1), (1, 0)])


def body(
    tokens,
    attn_gain,
    w_query,
    w_key,
    w_value,
    attn_bias,
    key_cache,
    value_cache,
    lengths,
    w_out,
    ffn_gain,
    routes,
    route_weight,
    expert_gate,
    expert_up,
    expert_down,
):
    seqs, width = tokens.shape
    half = width // 2
    top = routes.shape[1]
    experts = lax.axis_size("ep")
    copies = lax.axis_size("x")
    capacity = max(2, 2 * seqs * top // experts)
    blocks, out_rows, back_rows = sizes_of(capacity, half)
    bf = jnp.bfloat16
    pack, send, new_keys, new_values = attend(
        experts,
        capacity,
        tokens,
        attn_gain,
        w_query,
        w_key,
        w_value,
        attn_bias,
        key_cache,
        value_cache,
        lengths,
        w_out,
        routes,
        route_weight,
    )
    pad = -(-capacity // 8) * 8
    f32 = jnp.float32
    pick = local_call(
        functools.partial(pick_kernel, experts, out_rows, back_rows),
        jax.ShapeDtypeStruct((experts * out_rows, 2 * experts), bf),
        (),
        "pick",
        flops=5_000_000_000,
    )
    outgoing = local_call(
        functools.partial(scatter_kernel, capacity, top),
        jax.ShapeDtypeStruct((copies, experts, out_rows, LANES), bf),
        (pack, swap_core(send), pick),
        "scatter",
        flops=20_000_000_000,
    )
    arrived = lax.all_to_all(
        outgoing.reshape(copies * experts, out_rows, LANES), ("x", "ep"), 0, 0, tiled=True
    )
    mine = local_call(
        add_kernel,
        jax.ShapeDtypeStruct((experts, out_rows, LANES), bf),
        (arrived.reshape(copies, experts, out_rows, LANES),),
        "add",
    )
    theirs = swap_core(mine)
    hidden = expert_gate.shape[2]
    keep, send = local_call(
        functools.partial(expert_kernel, capacity, top * copies),
        (
            jax.ShapeDtypeStruct((experts, back_rows, LANES), f32),
            jax.ShapeDtypeStruct((experts, back_rows, LANES), bf),
        ),
        (
            mine,
            theirs,
            ffn_gain.reshape(1, -1),
            expert_gate[0],
            expert_up[0],
            expert_down[0],
        ),
        "experts",
        flops=6 * experts * capacity * width * hidden,
        scratch=(
            pltpu.VMEM((experts, out_rows, LANES), f32),
            pltpu.VMEM((experts, out_rows, LANES), f32),
            pltpu.VMEM((experts, pad, half), f32),
            pltpu.VMEM((experts, pad, half), f32),
            pltpu.VMEM((experts, back_rows, LANES), f32),
            pltpu.VMEM((experts, back_rows, LANES), f32),
        ),
    )
    part = (keep + swap_core(send).astype(jnp.float32)).astype(bf)
    part = jnp.broadcast_to(part[None], (copies, experts, back_rows, LANES))
    back = lax.all_to_all(
        part.reshape(copies * experts, back_rows, LANES), ("x", "ep"), 0, 0, tiled=True
    )
    mixed = local_call(
        functools.partial(gather_kernel, capacity, top),
        jax.ShapeDtypeStruct((seqs, half), bf),
        (pack, back.reshape(copies, experts, back_rows, LANES)),
        "gather",
    )
    other = swap_core(mixed)
    low_core = lax.axis_index("core") == 0
    mixed_rows = jnp.concatenate(
        [jnp.where(low_core, mixed, other), jnp.where(low_core, other, mixed)], axis=1
    )
    return (mixed_rows, new_keys, new_values)


def solution(mesh):
    experts, parts = mesh.devices.shape
    split = jax.sharding.Mesh(
        mesh.devices.reshape(experts, parts // 2, 2), ("ep", "x", "core")
    )
    tp = ("x", "core")
    return jax.shard_map(
        body,
        mesh=split,
        in_specs=(
            P("ep", None),
            P(),
            P(None, tp),
            P(None, tp),
            P(None, tp),
            P(tp),
            P("ep", tp, None),
            P("ep", tp, None),
            P("ep"),
            P(tp, None),
            P(),
            P("ep", None),
            P("ep", None),
            P("ep", None, tp),
            P("ep", None, tp),
            P("ep", tp, None),
        ),
        out_specs=(P("ep", None), P("ep", tp), P("ep", tp)),
        check_vma=False,
    )
```

```python
import functools

import jax
import jax.numpy as jnp
from jax import lax
from jax.experimental import pallas as pl
from jax.experimental.pallas import tpu as pltpu
from jax.sharding import PartitionSpec as P

HEAD = 64
norm_epsilon = 1e-06

LAST = (((1,), (1,)), ((), ()))


def iota(shape, axis):
    return lax.broadcasted_iota(jnp.int32, shape, axis)


def dot(a, b):
    return jnp.dot(a, b, preferred_element_type=jnp.float32)


def dot_last(a, b):
    return lax.dot_general(a, b, LAST, preferred_element_type=jnp.float32)


LANES = 128


def sizes_of(capacity, half):
    blocks = half // LANES
    back = -(-(capacity * blocks) // 8) * 8
    return blocks, back + 8, back


def plan_rows(experts, capacity, blocks, out_rows, back_rows, routes, shares):
    top, seqs = routes.shape
    owner = iota((experts, seqs), 0)
    hits = [(owner == routes[k : k + 1, :]).astype(jnp.float32) for k in range(top)]
    any_hit = sum(hits[1:], hits[0])
    earlier = (iota((seqs, seqs), 0) < iota((seqs, seqs), 1)).astype(jnp.bfloat16)
    before = dot(any_hit.astype(jnp.bfloat16), earlier)
    eye = (iota((seqs, seqs), 0) == iota((seqs, seqs), 1)).astype(jnp.bfloat16)
    targets = []
    high_mix = jnp.zeros((experts, LANES), jnp.float32)
    low_mix = jnp.zeros((experts, LANES), jnp.float32)
    for k in range(top):
        slot = jnp.sum(hits[k] * before, axis=0, keepdims=True)
        expert = routes[k : k + 1, :].astype(jnp.float32)
        for rows in (out_rows, back_rows):
            first = expert * rows + slot
            wide = jnp.concatenate([first + b * capacity for b in range(blocks)], axis=1)
            targets.append(wide)
        spread = jnp.broadcast_to(slot, (8, seqs)).astype(jnp.bfloat16)
        column = dot_last(eye, spread)[:, :1].astype(jnp.int32)
        at = (iota((seqs, LANES), 1) == column).astype(jnp.bfloat16)
        share = hits[k] * shares[k : k + 1, :]
        high = share.astype(jnp.bfloat16)
        low = (share - high.astype(jnp.float32)).astype(jnp.bfloat16)
        high_mix = high_mix + dot(high, at)
        low_mix = low_mix + dot(low, at)
    return targets, high_mix, low_mix


def plan_of(pack_ref, seqs, top, blocks, total, way):
    row = iota((total, blocks * seqs), 0)
    plan = jnp.zeros((total, blocks * seqs), jnp.float32)
    for k in range(top):
        at = seqs + 2 * k + way
        target = pack_ref[at : at + 1, : blocks * seqs].astype(jnp.int32)
        plan = plan + (row == target).astype(jnp.float32)
    return plan.astype(jnp.bfloat16)


def pick_kernel(experts, rows, back_rows, pick_ref):
    line, col = iota(pick_ref.shape, 0), iota((1, pick_ref.shape[1]), 1)
    want = (col % experts) * rows + back_rows + col // experts
    pick_ref[...] = (line == want).astype(jnp.float32).astype(jnp.bfloat16)


def attend_kernel(
    group,
    experts,
    capacity,
    lengths_hbm,
    bias_hbm,
    tokens_hbm,
    gain_hbm,
    wq_hbm,
    wk_hbm,
    wv_hbm,
    wo_hbm,
    key_hbm,
    value_hbm,
    route_hbm,
    weight_hbm,
    pack_ref,
    send_ref,
    new_key_ref,
    new_value_ref,
    lengths,
    bias,
    tokens_ref,
    gain_ref,
    wq_ref,
    wk_ref,
    wv_ref,
    wo_ref,
    key_ref,
    value_ref,
    route_ref,
    weight_ref,
    small_sem,
    key_sem,
    value_sem,
):
    seqs = tokens_ref.shape[0]
    span = key_ref.shape[1]
    heads = wq_ref.shape[1] // HEAD
    depth = group * HEAD
    rows = group * heads
    count = seqs // group
    early = (
        (tokens_hbm, tokens_ref),
        (gain_hbm, gain_ref),
        (wq_hbm, wq_ref),
        (lengths_hbm, lengths),
        (bias_hbm, bias),
        (route_hbm, route_ref),
        (weight_hbm, weight_ref),
    )
    late = ((wk_hbm, wk_ref), (wv_hbm, wv_ref), (wo_hbm, wo_ref))
    copies = [
        pltpu.make_async_copy(src, dst, small_sem.at[i])
        for i, (src, dst) in enumerate(early + late)
    ]
    fetched, last = copies[: len(early)], copies[len(early) :]

    def chunk(src, dst, sem, g):
        part = pl.ds(g * depth, depth)
        return pltpu.make_async_copy(src.at[part], dst.at[part], sem.at[g])

    stream = [chunk(key_hbm, key_ref, key_sem, g) for g in range(count)]
    stream += last
    stream += [chunk(value_hbm, value_ref, value_sem, g) for g in range(count)]
    started = [0]

    def start_to(limit):
        while started[0] < min(limit, len(stream)):
            stream[started[0]].start()
            started[0] += 1

    for copy in fetched:
        copy.start()
    start_to(max(1, count - 2))
    fetched[0].wait()
    fetched[1].wait()
    start_to(count)
    widened = tokens_ref[...].astype(jnp.float32)
    factor = lax.rsqrt(jnp.mean(widened * widened, axis=-1, keepdims=True) + norm_epsilon)
    normed = (widened * factor * gain_ref[...]).astype(jnp.bfloat16)
    for copy in fetched[2:]:
        copy.wait()
    start_to(len(stream))
    queries = dot(normed, wq_ref[...]).astype(jnp.bfloat16)

    total = seqs * heads
    spread = jnp.zeros((total, HEAD), jnp.float32)
    r0, c0 = iota((total, seqs), 0), iota((total, seqs), 1)
    for h in range(heads):
        pick = (r0 == c0 * heads + h).astype(jnp.bfloat16)
        spread = spread + dot(pick, queries[:, h * HEAD : (h + 1) * HEAD])
    tiled = jnp.concatenate([spread.astype(jnp.bfloat16)] * group, axis=1)
    r1, c1 = iota((total, depth), 0), iota((total, depth), 1)
    own = (r1 // heads) % group == c1 // HEAD
    stacked = jnp.where(own, tiled, jnp.zeros_like(tiled))

    block = min(256, span)
    blocks = span // block
    tri = (iota((block, block), 0) >= iota((block, block), 1)).astype(jnp.bfloat16)
    row_id = iota((rows, 1), 0)
    bias_col = jnp.zeros((rows, 1), jnp.float32)
    for h in range(heads):
        bias_col = jnp.where(row_id % heads == h, bias[h], bias_col)
    place = iota((rows, span), 1)

    inside, scored, sums, weights, pieces = {}, {}, {}, {}, {}
    cuts = [slice(b * block, (b + 1) * block) for b in range(blocks)]

    def score(g):
        scores = dot(stacked[g * rows : (g + 1) * rows], key_ref[pl.ds(g * depth, depth), :])
        scores = scores * HEAD ** (-0.5) + bias_col
        length = jnp.zeros((rows, 1), jnp.int32)
        for j in range(group):
            length = jnp.where(row_id // heads == j, lengths[g * group + j], length)
        inside[g] = place < length
        fall = jnp.maximum(scores, 0.0) + jnp.log(1.0 + jnp.exp(-jnp.abs(scores)))
        fall = jnp.where(inside[g], -fall, 0.0)
        high = fall.astype(jnp.bfloat16)
        low = (fall - high.astype(jnp.float32)).astype(jnp.bfloat16)
        both = jnp.concatenate([high[:, c] for c in cuts] + [low[:, c] for c in cuts], axis=0)
        scored[g] = scores
        sums[g] = dot(both, tri)

    def weigh(g):
        later = jnp.zeros((rows, 1), jnp.float32)
        after = [None] * blocks
        for b in reversed(range(blocks)):
            within = (
                sums[g][b * rows : (b + 1) * rows]
                + sums[g][(blocks + b) * rows : (blocks + b + 1) * rows]
            )
            after[b] = within + later
            later = later + within[:, :1]
        weights[g] = jnp.where(
            inside[g], jnp.exp(scored[g] + jnp.concatenate(after, axis=1)), 0.0
        ).astype(jnp.bfloat16)

    def read(g):
        pieces[g] = dot_last(weights[g], value_ref[pl.ds(g * depth, depth), :])

    blocks_out, out_rows, back_rows = sizes_of(capacity, pack_ref.shape[1])
    targets, high_mix, low_mix = plan_rows(
        experts, capacity, blocks_out, out_rows, back_rows, route_ref[...], weight_ref[...]
    )
    pack_ref[seqs:, :] = jnp.zeros((pack_ref.shape[0] - seqs, pack_ref.shape[1]), jnp.float32)
    for k, target in enumerate(targets):
        pack_ref[seqs + k : seqs + k + 1, : target.shape[1]] = target
    base_row = seqs + 8
    pack_ref[base_row : base_row + experts, :LANES] = high_mix
    pack_ref[base_row + experts : base_row + 2 * experts, :LANES] = low_mix
    for copy in stream[:count]:
        copy.wait()
    for g in range(count):
        score(g)
    for g in range(count):
        weigh(g)
    for copy in last:
        copy.wait()
    new_key_ref[...] = dot_last(normed, wk_ref[...]).astype(jnp.bfloat16)
    new_value_ref[...] = dot_last(normed, wv_ref[...]).astype(jnp.bfloat16)
    for copy in stream[count + len(last) :]:
        copy.wait()
    for g in range(count):
        read(g)
    mixed = jnp.where(own, jnp.concatenate([pieces[g] for g in range(count)], axis=0), 0.0)
    folded = mixed[:, :HEAD]
    for j in range(1, group):
        folded = folded + mixed[:, j * HEAD : (j + 1) * HEAD]
    folded = folded.astype(jnp.bfloat16)
    r2, c2 = iota((seqs, total), 0), iota((seqs, total), 1)
    attended = jnp.concatenate(
        [dot((c2 == r2 * heads + h).astype(jnp.bfloat16), folded) for h in range(heads)], axis=1
    ).astype(jnp.bfloat16)
    out = dot(attended, wo_ref[...])
    half = out.shape[1] // 2
    low_core = lax.axis_index("core") == 0
    first = lax.axis_index("x") == 0
    keep = jnp.where(low_core, out[:, :half], out[:, half:])
    base = jnp.where(low_core, widened[:, :half], widened[:, half:])
    pack_ref[:seqs, :] = keep + jnp.where(first, base, jnp.zeros_like(base))
    send_ref[...] = jnp.where(low_core, out[:, half:], out[:, :half]).astype(jnp.bfloat16)


def attend(
    experts, capacity, tokens, gain, wq, wk, wv, bias, keys, values, lengths, wo, routes, shares
):
    seqs, width = tokens.shape
    head_cols = wq.shape[1]
    kv_cols = wk.shape[1]
    assert kv_cols == HEAD
    span = keys.shape[2]
    top = routes.shape[1]
    group = 256 // HEAD
    while seqs % group:
        group //= 2
    hbm = pl.BlockSpec(memory_space=pltpu.HBM)
    vmem = pl.BlockSpec(memory_space=pltpu.VMEM)
    count = seqs // group
    bf = jnp.bfloat16
    return pl.pallas_call(
        functools.partial(attend_kernel, group, experts, capacity),
        out_shape=(
            jax.ShapeDtypeStruct((seqs + 8 + 2 * experts, width // 2), jnp.float32),
            jax.ShapeDtypeStruct((seqs, width // 2), bf),
            jax.ShapeDtypeStruct((seqs, kv_cols), bf),
            jax.ShapeDtypeStruct((seqs, kv_cols), bf),
        ),
        in_specs=[hbm] * 12,
        out_specs=(vmem,) * 4,
        scratch_shapes=[
            pltpu.SMEM((seqs,), jnp.int32),
            pltpu.SMEM((head_cols // HEAD,), jnp.float32),
            pltpu.VMEM((seqs, width), bf),
            pltpu.VMEM((1, width), jnp.float32),
            pltpu.VMEM((width, head_cols), bf),
            pltpu.VMEM((kv_cols, width), bf),
            pltpu.VMEM((kv_cols, width), bf),
            pltpu.VMEM((head_cols, width), bf),
            pltpu.VMEM((seqs * kv_cols, span), bf),
            pltpu.VMEM((seqs * kv_cols, span), bf),
            pltpu.VMEM((top, seqs), jnp.int32),
            pltpu.VMEM((top, seqs), jnp.float32),
            pltpu.SemaphoreType.DMA((10,)),
            pltpu.SemaphoreType.DMA((count,)),
            pltpu.SemaphoreType.DMA((count,)),
        ],
        compiler_params=pltpu.CompilerParams(vmem_limit_bytes=67043328),
        cost_estimate=pl.CostEstimate(
            flops=4 * seqs * head_cols * span + 4 * seqs * width * head_cols,
            bytes_accessed=4 * seqs * kv_cols * span + 4 * width * head_cols,
            transcendentals=3 * seqs * head_cols // HEAD * span,
        ),
        name="attend",
    )(
        lengths,
        bias,
        tokens,
        gain.reshape(1, -1),
        wq,
        wk.T,
        wv.T,
        wo,
        keys.reshape(seqs * kv_cols, span),
        values.reshape(seqs * kv_cols, span),
        routes.T,
        shares.T,
    )


def stacked_blocks(value, blocks):
    return jnp.concatenate([value[:, b * LANES : (b + 1) * LANES] for b in range(blocks)], axis=0)


def unstacked(value, blocks):
    rows = value.shape[0] // blocks
    return [value[b * rows : (b + 1) * rows] for b in range(blocks)]


def scatter_kernel(capacity, top, pack_ref, got_ref, pick_ref, out_ref):
    copies, experts, rows, lanes = out_ref.shape
    seqs, half = got_ref.shape
    blocks = half // lanes
    total = experts * rows
    summed = (pack_ref[:seqs, :] + got_ref[...].astype(jnp.float32)).astype(jnp.bfloat16)
    placed = dot(plan_of(pack_ref, seqs, top, blocks, total, 0), stacked_blocks(summed, blocks))
    mixes = pack_ref[seqs + 8 : seqs + 8 + 2 * experts, :lanes].astype(jnp.bfloat16)
    whole = (placed + dot(pick_ref[...], mixes) * (1.0 / copies)).astype(jnp.bfloat16)
    whole = whole.reshape(experts, rows, lanes)
    for copy in range(copies):
        out_ref[copy] = whole


def add_kernel(arrived_ref, out_ref):
    whole = arrived_ref[0].astype(jnp.float32)
    for copy in range(1, arrived_ref.shape[0]):
        whole = whole + arrived_ref[copy].astype(jnp.float32)
    out_ref[...] = whole.astype(jnp.bfloat16)


def join_kernel(keep_ref, got_ref, out_ref):
    whole = (keep_ref[...] + got_ref[...].astype(jnp.float32)).astype(jnp.bfloat16)
    for copy in range(out_ref.shape[0]):
        out_ref[copy] = whole


def expert_kernel(
    capacity,
    copies,
    mine_ref,
    theirs_ref,
    gain_ref,
    gate_ref,
    up_ref,
    down_ref,
    keep_ref,
    send_ref,
    mine_rows,
    theirs_rows,
    left_ref,
    right_ref,
    keep_rows,
    send_rows,
):
    sources, _, lanes = mine_ref.shape
    back_rows = keep_ref.shape[1]
    half = left_ref.shape[2]
    pad = left_ref.shape[1]
    blocks = half // lanes
    total = sources * pad
    low_core = lax.axis_index("core") == 0
    mine_rows[...] = mine_ref[...].astype(jnp.float32)
    theirs_rows[...] = theirs_ref[...].astype(jnp.float32)
    if pad > capacity:
        rest = jnp.zeros((sources, pad - capacity, half), jnp.float32)
        left_ref[:, capacity:, :] = rest
        right_ref[:, capacity:, :] = rest
    for b in range(blocks):
        chunk = slice(b * capacity, (b + 1) * capacity)
        cols = slice(b * lanes, (b + 1) * lanes)
        a, c = mine_rows[:, chunk, :], theirs_rows[:, chunk, :]
        left_ref[:, :capacity, cols] = jnp.where(low_core, a, c)
        right_ref[:, :capacity, cols] = jnp.where(low_core, c, a)
    left = left_ref[...].reshape(total, half)
    right = right_ref[...].reshape(total, half)
    residual = jnp.concatenate([left, right], axis=1)
    factor = lax.rsqrt(jnp.mean(residual * residual, axis=-1, keepdims=True) + norm_epsilon)
    normed = (residual * factor * gain_ref[...]).astype(jnp.bfloat16)
    units = gate_ref.shape[1]
    pieces = []
    for start in range(0, units, 256):
        part = slice(start, min(start + 256, units))
        gated = dot(normed, gate_ref[:, part])
        lifted = dot(normed, up_ref[:, part])
        pieces.append((gated / (1.0 + jnp.exp(-gated)) * lifted).astype(jnp.bfloat16))
    out = dot(jnp.concatenate(pieces, axis=1), down_ref[...])
    share = mine_rows[:, back_rows : back_rows + 1, :] + mine_rows[:, back_rows + 1 : back_rows + 2, :]
    share = jnp.broadcast_to(share, (sources, pad, lanes)).reshape(total, lanes)
    at_slot = iota((total, lanes), 1) == iota((total, lanes), 0) % pad
    share = jnp.sum(jnp.where(at_slot, share, 0.0), axis=1, keepdims=True)
    own = jnp.where(low_core, out[:, :half], out[:, half:]) * share
    own = own + jnp.where(low_core, left, right) * (1.0 / copies)
    other = jnp.where(low_core, out[:, half:], out[:, :half]) * share
    own = own.reshape(sources, pad, half)
    other = other.reshape(sources, pad, half)
    if back_rows > blocks * capacity:
        rest = jnp.zeros((sources, back_rows - blocks * capacity, lanes), jnp.float32)
        keep_rows[:, blocks * capacity :, :] = rest
        send_rows[:, blocks * capacity :, :] = rest
    for b in range(blocks):
        chunk = slice(b * capacity, (b + 1) * capacity)
        cols = slice(b * lanes, (b + 1) * lanes)
        keep_rows[:, chunk, :] = own[:, :capacity, cols]
        send_rows[:, chunk, :] = other[:, :capacity, cols]
    keep_ref[...] = keep_rows[...]
    send_ref[...] = send_rows[...].astype(jnp.bfloat16)


def gather_kernel(capacity, top, pack_ref, back_ref, out_ref):
    copies, experts, rows, lanes = back_ref.shape
    seqs, half = out_ref.shape
    blocks = half // lanes
    plan = plan_of(pack_ref, seqs, top, blocks, experts * rows, 1)
    out = jnp.zeros((blocks * seqs, lanes), jnp.float32)
    for copy in range(copies):
        block = back_ref[copy].reshape(experts * rows, lanes)
        out = out + lax.dot_general(
            plan, block, (((0,), (0,)), ((), ())), preferred_element_type=jnp.float32
        )
    out_ref[...] = jnp.concatenate(unstacked(out, blocks), axis=1).astype(jnp.bfloat16)


def local_call(kernel, outs, args, name, limit=16, flops=0, scratch=()):
    vmem = pl.BlockSpec(memory_space=pltpu.VMEM)
    moved = sum(a.size * a.dtype.itemsize for a in args)
    return pl.pallas_call(
        kernel,
        out_shape=outs,
        in_specs=[vmem] * len(args),
        out_specs=jax.tree.map(lambda _: vmem, outs),
        scratch_shapes=scratch,
        compiler_params=pltpu.CompilerParams(vmem_limit_bytes=limit * 1024 * 1024),
        cost_estimate=pl.CostEstimate(flops=flops, bytes_accessed=moved, transcendentals=0),
        name=name,
    )(*args)


def swap_core(value):
    return lax.ppermute(value, "core", [(0, 1), (1, 0)])


def body(
    tokens,
    attn_gain,
    w_query,
    w_key,
    w_value,
    attn_bias,
    key_cache,
    value_cache,
    lengths,
    w_out,
    ffn_gain,
    routes,
    route_weight,
    expert_gate,
    expert_up,
    expert_down,
):
    seqs, width = tokens.shape
    half = width // 2
    top = routes.shape[1]
    experts = lax.axis_size("ep")
    copies = lax.axis_size("x")
    capacity = max(2, 2 * seqs * top // experts)
    blocks, out_rows, back_rows = sizes_of(capacity, half)
    bf = jnp.bfloat16
    pack, send, new_keys, new_values = attend(
        experts,
        capacity,
        tokens,
        attn_gain,
        w_query,
        w_key,
        w_value,
        attn_bias,
        key_cache,
        value_cache,
        lengths,
        w_out,
        routes,
        route_weight,
    )
    pad = -(-capacity // 8) * 8
    f32 = jnp.float32
    pick = local_call(
        functools.partial(pick_kernel, experts, out_rows, back_rows),
        jax.ShapeDtypeStruct((experts * out_rows, 2 * experts), bf),
        (),
        "pick",
        flops=5_000_000_000,
    )
    outgoing = local_call(
        functools.partial(scatter_kernel, capacity, top),
        jax.ShapeDtypeStruct((copies, experts, out_rows, LANES), bf),
        (pack, swap_core(send), pick),
        "scatter",
        flops=20_000_000_000,
    )
    arrived = lax.all_to_all(
        outgoing.reshape(copies * experts, out_rows, LANES), ("x", "ep"), 0, 0, tiled=True
    )
    mine = local_call(
        add_kernel,
        jax.ShapeDtypeStruct((experts, out_rows, LANES), bf),
        (arrived.reshape(copies, experts, out_rows, LANES),),
        "add",
    )
    theirs = swap_core(mine)
    hidden = expert_gate.shape[2]
    keep, send = local_call(
        functools.partial(expert_kernel, capacity, top * copies),
        (
            jax.ShapeDtypeStruct((experts, back_rows, LANES), f32),
            jax.ShapeDtypeStruct((experts, back_rows, LANES), bf),
        ),
        (
            mine,
            theirs,
            ffn_gain.reshape(1, -1),
            expert_gate[0],
            expert_up[0],
            expert_down[0],
        ),
        "experts",
        flops=6 * experts * capacity * width * hidden,
        scratch=(
            pltpu.VMEM((experts, out_rows, LANES), f32),
            pltpu.VMEM((experts, out_rows, LANES), f32),
            pltpu.VMEM((experts, pad, half), f32),
            pltpu.VMEM((experts, pad, half), f32),
            pltpu.VMEM((experts, back_rows, LANES), f32),
            pltpu.VMEM((experts, back_rows, LANES), f32),
        ),
    )
    part = local_call(
        join_kernel,
        jax.ShapeDtypeStruct((copies, experts, back_rows, LANES), bf),
        (keep, swap_core(send)),
        "join",
    )
    back = lax.all_to_all(
        part.reshape(copies * experts, back_rows, LANES), ("x", "ep"), 0, 0, tiled=True
    )
    mixed = local_call(
        functools.partial(gather_kernel, capacity, top),
        jax.ShapeDtypeStruct((seqs, half), bf),
        (pack, back.reshape(copies, experts, back_rows, LANES)),
        "gather",
    )
    other = swap_core(mixed)
    low_core = lax.axis_index("core") == 0
    mixed_rows = jnp.concatenate(
        [jnp.where(low_core, mixed, other), jnp.where(low_core, other, mixed)], axis=1
    )
    return (mixed_rows, new_keys, new_values)


def solution(mesh):
    experts, parts = mesh.devices.shape
    split = jax.sharding.Mesh(
        mesh.devices.reshape(experts, parts // 2, 2), ("ep", "x", "core")
    )
    tp = ("x", "core")
    return jax.shard_map(
        body,
        mesh=split,
        in_specs=(
            P("ep", None),
            P(),
            P(None, tp),
            P(None, tp),
            P(None, tp),
            P(tp),
            P("ep", tp, None),
            P("ep", tp, None),
            P("ep"),
            P(tp, None),
            P(),
            P("ep", None),
            P("ep", None),
            P("ep", None, tp),
            P("ep", None, tp),
            P("ep", tp, None),
        ),
        out_specs=(P("ep", None), P("ep", tp), P("ep", tp)),
        check_vma=False,
    )
```
